32 devices in a mesh: sp: 16 (over z, y, x), tp: 2 (over core).
Axes of the slice: x: 2, y: 2, z: 4, core: 2. Of those that a mesh axis runs over, the one named last changes fastest.
Arguments:
- head_value_rows: bfloat16 [12288, 2048], P('sp', 'tp'), may hold values from -6 to 6
- entry_map_rows: bfloat16 [12288, 1024], P('sp', 'tp'), may hold values from -6 to 6
- readout_map_rows: bfloat16 [12288, 1024], P('sp', 'tp'), may hold values from -6 to 6
- output_gate_rows: bfloat16 [12288, 2048], P('sp', 'tp'), may hold values from -6 to 6
- step_before_softplus: bfloat16 [12288, 32], P('sp', 'tp'), may hold values from -8 to 8
- sudden_log_decay: float32 [12288, 32], P('sp', 'tp'), may hold values from -1 to 0
- document_index: int32 [12288], replicated, may hold values from 0 to 3, never falling along the last dimension, each value on 1 to 6144 neighbouring positions
- head_rate_logarithm: float32 [2, 32], P(None, 'tp'), may hold values from -30 to 0
- head_step_bias: float32 [2, 32], P(None, 'tp'), may hold values from -3 to 3
- value_conv_taps: bfloat16 [5, 2048], P(None, 'tp'), may hold values from -2.5 to 2.5
- entry_conv_taps: bfloat16 [5, 1024], P(None, 'tp'), may hold values from -2.5 to 2.5
- readout_conv_taps: bfloat16 [5, 1024], P(None, 'tp'), may hold values from -2.5 to 2.5
- group_norm_gain: float32 [2048], P('tp'), may hold values from 0.1 to 1.9
- mixer_output_weight: bfloat16 [2048, 2048], P('tp'), may hold values from -0.125 to 0.125
- stream: bfloat16 [12288, 2048], P('sp', 'tp'), may hold values from -200 to 200
- mixer_norm_gain: float32 [2048], P('tp'), may hold values from 0.1 to 1.9
- channel_norm_gain: float32 [2048], P('tp'), may hold values from 0.1 to 1.9
- up_projection_weight: bfloat16 [2048, 8192], P('sp', 'tp'), may hold values from -0.125 to 0.125
- down_projection_weight: bfloat16 [2048, 8192], P('sp', 'tp'), may hold values from -0.0625 to 0.0625
Outputs:
- mixed: bfloat16 [12288, 2048], P('sp', 'tp')
The draws below stay inside these ranges and needn't reach their ends.
All inputs are finite; a program needn't handle non-finite values.
Results may differ from the reference program's by a relative error of at most 0.018.
Values may be sent and summed in bfloat16 or wider, within the bound.
A program may use at most 128 MiB of HBM per device.

```python
import math
import jax
import jax.numpy as jnp
import numpy as np
from jax import lax

D = 2048
HEADS = 32
HEAD_DIM = 64
GROUPS = 8
STATE = 128
FF = 8192
CONV_WIDTH = 5
BLOCK = 128
TOK_DEV = 768
INNER = 2048
TOKENS = 12288
N_SP = 16
N_TP = 2


def draw_step_before_softplus(key, part):
    jitter_key, shift_key = jax.random.split(key)
    jitter = jnp.clip(jax.random.normal(jitter_key, (TOKENS, HEADS), jnp.float32), -4.0, 4.0)
    shifts = jax.random.uniform(shift_key, (TOKENS // TOK_DEV, 1, HEADS), jnp.float32, -1.0, 1.5)
    shifts = jnp.broadcast_to(shifts, (TOKENS // TOK_DEV, TOK_DEV, HEADS)).reshape(TOKENS, HEADS)
    return (jitter + shifts).astype(jnp.bfloat16)


def draw_head_rate_logarithm(key, part):
    pick_key, slow_key, fast_key = jax.random.split(key, 3)
    quick = jax.random.randint(pick_key, (2, HEADS), 0, 2) == 1
    slow_rate = jax.random.uniform(slow_key, (2, HEADS), jnp.float32, math.log(0.1), math.log(0.5))
    slow_rate = slow_rate - jnp.log(jnp.float32(TOKENS))
    fast_rate = jax.random.uniform(fast_key, (2, HEADS), jnp.float32, math.log(0.01), math.log(1.0 / 30.0))
    return jnp.where(quick, fast_rate, slow_rate)


def draw_sudden_log_decay(key, part):
    where_key, depth_key = jax.random.split(key)
    struck = jax.random.randint(where_key, (TOKENS, 1), 0, TOKENS) < 4
    depth = jax.random.uniform(depth_key, (TOKENS, HEADS), jnp.float32, math.log(0.5), math.log(0.8))
    return jnp.where(struck, depth, 0.0)


def draw_stream(key, part):
    base_key, row_key = jax.random.split(key, 2)
    col_scale = 3.0 ** (jnp.arange(D, dtype=jnp.float32) / D - 0.5)
    values = jnp.clip(jax.random.normal(base_key, (TOKENS, D), jnp.float32), -6.0, 6.0)
    row_scale = jnp.exp(jax.random.uniform(row_key, (TOKENS, 1), jnp.float32, math.log(0.5), math.log(2.0)))
    return (values * row_scale * col_scale).astype(jnp.bfloat16)


def levels(stream_key, shape, cuts, low, largest):
    loudness = 1.0
    for axis_at, blocks in cuts:
        heights = jax.random.uniform(jax.random.fold_in(jax.random.fold_in(stream_key, 6), axis_at), (blocks,), jnp.float32, low / len(cuts), largest / len(cuts))
        loudness = loudness * jnp.repeat(jnp.exp(heights), shape[axis_at] // blocks).reshape((-1,) + (1,) * (len(shape) - 1 - axis_at))
    return loudness


def split_up(amount, total, bound, skew):
    weights = [(1 << 20) // math.isqrt(grade ** skew) + 1 for grade in range(2, amount + 1)]
    spare, holding = total - bound - (amount - 1), [1] * (amount - 1)
    while spare > 0:
        movable = [i for i in range(amount - 1) if holding[i] < bound]
        pool, remaining = sum([weights[i] for i in movable]), spare
        for i in movable:
            more = min(bound - holding[i], max(1, remaining * weights[i] // pool), spare)
            holding[i] = holding[i] + more
            spare = spare - more
    return np.array([bound] + holding)


def ragged_sizes(key, amount, total, reach, skew):
    if amount == 2:
        one = jax.random.randint(key, (), max(1, total - reach), min(reach, total - 1) + 1)
        return jnp.stack([one, total - one])
    sizes = jnp.asarray(split_up(amount, total, reach, skew), jnp.int32)
    twos = (amount - 1) // 2
    donor, receiver = sizes[1:1 + 2 * twos:2], sizes[2:2 + 2 * twos:2]
    margin = jnp.minimum(donor - 1, reach - receiver)
    shifted = jax.random.randint(jax.random.fold_in(key, 1), (twos,), 0, 1 << 20) % (margin + 1)
    sizes = sizes.at[1:1 + 2 * twos:2].set(donor - shifted).at[2:2 + 2 * twos:2].set(receiver + shifted)
    return sizes[jax.random.permutation(jax.random.fold_in(key, 2), amount)]


def noise(own_key, extent, deviation, most, cuts=(), kind=jnp.bfloat16):
    loudness = levels(own_key, extent, cuts, -0.22, 0.18) if cuts else 1.0
    values = jax.random.normal(own_key, extent, jnp.float32) * deviation * loudness
    return jnp.minimum(jnp.maximum(values, -most), most).astype(kind)


def setup_inputs(seed: int = 0) -> dict:
    arg_keys = jax.random.split(jax.random.key(seed), 20)
    return {
        "head_value_rows": noise(arg_keys[0], (TOKENS, INNER), 1.0, 6.0, ((0, 16), (1, 2))),
        "entry_map_rows": noise(arg_keys[1], (TOKENS, GROUPS * STATE), 1.0, 6.0, ((0, 16), (1, 2))),
        "readout_map_rows": noise(arg_keys[2], (TOKENS, GROUPS * STATE), 1.0, 6.0, ((0, 16), (1, 2))),
        "output_gate_rows": noise(arg_keys[3], (TOKENS, INNER), 1.0, 6.0, ((0, 16), (1, 2))),
        "step_before_softplus": draw_step_before_softplus(jax.random.fold_in(arg_keys[19], 71), 0),
        "sudden_log_decay": draw_sudden_log_decay(jax.random.fold_in(arg_keys[19], 71), 0),
        "document_index": jnp.searchsorted(jnp.cumsum(ragged_sizes(arg_keys[6], N_SP // 4, TOKENS, 8 * TOK_DEV, 1)), jnp.arange(TOKENS), side="right").astype(jnp.int32),
        "head_rate_logarithm": draw_head_rate_logarithm(jax.random.fold_in(arg_keys[19], 71), 0),
        "head_step_bias": noise(arg_keys[8], (2, HEADS), 0.5, 3.0, ((1, 2),), jnp.float32),
        "value_conv_taps": noise(arg_keys[9], (CONV_WIDTH, INNER), CONV_WIDTH ** -0.5, 2.5, ((1, 2),)),
        "entry_conv_taps": noise(arg_keys[10], (CONV_WIDTH, GROUPS * STATE), CONV_WIDTH ** -0.5, 2.5, ((1, 2),)),
        "readout_conv_taps": noise(arg_keys[11], (CONV_WIDTH, GROUPS * STATE), CONV_WIDTH ** -0.5, 2.5, ((1, 2),)),
        "group_norm_gain": jnp.clip(1.0 + 0.18 * jax.random.normal(arg_keys[12], (INNER,), jnp.float32), 0.1, 1.9),
        "mixer_output_weight": noise(arg_keys[13], (INNER, D), INNER ** -0.5, 0.125, ((0, 2),)),
        "stream": draw_stream(jax.random.fold_in(arg_keys[19], 71), 0),
        "mixer_norm_gain": jnp.clip(1.0 + 0.18 * jax.random.normal(arg_keys[15], (D,), jnp.float32), 0.1, 1.9),
        "channel_norm_gain": jnp.clip(1.0 + 0.18 * jax.random.normal(arg_keys[16], (D,), jnp.float32), 0.1, 1.9),
        "up_projection_weight": noise(arg_keys[17], (D, FF), D ** -0.5, 0.125, ((0, 16), (1, 2))),
        "down_projection_weight": noise(arg_keys[18], (D, FF), FF ** -0.5, 0.0625, ((0, 16), (1, 2))),
    }


exact_prec = lax.Precision.HIGHEST
norm_eps = 1e-05
resid_scale = 1.4142135623730951

def block_step(running, blocks):
    states, last_doc = running
    scaled, entries, readout, decay_logarithm, block_ids = blocks
    block_len = block_ids.shape[0]
    cum_decay = jnp.cumsum(decay_logarithm, axis=0)
    indices = lax.iota(jnp.int32, block_len)
    linked = (indices[:, None] >= indices[None, :]) & (block_ids[:, None] == block_ids[None, :])
    link_mask = linked[:, :, None, None]
    spread = cum_decay[:, None] - cum_decay[None, :]
    weights = jnp.where(link_mask, jnp.exp(jnp.where(link_mask, spread, 0.0)), 0.0)
    scores = jnp.einsum('tgn,sgn->tsg', readout, entries, precision=exact_prec)
    within = jnp.einsum('tsg,tsgr,sgrp->tgrp', scores, weights, scaled, precision=exact_prec)
    arrival = jnp.where((block_ids == last_doc)[:, None, None], jnp.exp(cum_decay), 0.0)
    carried = jnp.einsum('tgn,grpn->tgrp', readout, states, precision=exact_prec) * arrival[..., None]
    end_doc = block_ids[-1]
    to_end = jnp.where((block_ids == end_doc)[:, None, None], jnp.exp(cum_decay[-1] - cum_decay), 0.0)
    passing = jnp.where(end_doc == last_doc, jnp.exp(cum_decay[-1]), 0.0)
    fresh = jnp.einsum('sgn,sgr,sgrp->grpn', entries, to_end, scaled, precision=exact_prec)
    return ((states * passing[..., None, None] + fresh, end_doc), within + carried)

def sweep_blocks(scaled, entries, readout, decay_logarithm, document_index, states, last_doc, block_len):
    row_count = document_index.shape[0]
    block_count = row_count // block_len

    def in_blocks(array):
        return array.reshape((block_count, block_len) + array.shape[1:])
    inputs = tuple((in_blocks(array) for array in (scaled, entries, readout, decay_logarithm, document_index)))
    (states, last_doc), output = lax.scan(block_step, (states, last_doc), inputs)
    return (output.reshape((row_count,) + output.shape[2:]), states)

def short_conv(inputs, weights, document_index):
    taps = weights.shape[0]
    half_width = taps // 2
    row_count = inputs.shape[0]
    padded = jnp.pad(inputs, ((half_width, half_width), (0, 0)))
    doc_pad = jnp.pad(document_index, half_width, constant_values=-1)
    summed = jnp.zeros(inputs.shape, jnp.float32)
    for offset in range(taps):
        same_doc = (doc_pad[offset:offset + row_count] == document_index)[:, None]
        summed = summed + weights[offset] * jnp.where(same_doc, padded[offset:offset + row_count], 0.0)
    return jax.nn.silu(summed)

def layer_norm(residual, gain):
    row_mean = lax.optimization_barrier(jnp.mean(residual, axis=1))
    row_var = lax.optimization_barrier(jnp.mean(residual * residual, axis=1)) - row_mean * row_mean
    return ((residual - row_mean[:, None]) * lax.rsqrt(row_var + norm_eps)[:, None] * gain).astype(jnp.bfloat16)

def block_sums(left, right):
    parts = jnp.einsum('tjc,jcd->jtd', left, right)
    rounded = parts.astype(jnp.bfloat16)
    rounded = lax.optimization_barrier(rounded)
    return lax.optimization_barrier(jnp.sum(rounded.astype(jnp.float32), axis=0))

def reference(head_value_rows, entry_map_rows, readout_map_rows, output_gate_rows, step_before_softplus, sudden_log_decay, document_index, head_rate_logarithm, head_step_bias, value_conv_taps, entry_conv_taps, readout_conv_taps, group_norm_gain, mixer_output_weight, stream, mixer_norm_gain, channel_norm_gain, up_projection_weight, down_projection_weight):
    per_group = HEADS // GROUPS
    values = short_conv(head_value_rows.astype(jnp.float32), value_conv_taps.astype(jnp.float32), document_index)
    values = values.reshape(TOKENS, GROUPS, per_group, HEAD_DIM)
    entries = short_conv(entry_map_rows.astype(jnp.float32), entry_conv_taps.astype(jnp.float32), document_index)
    entries = entries.reshape(TOKENS, GROUPS, STATE)
    readout = short_conv(readout_map_rows.astype(jnp.float32), readout_conv_taps.astype(jnp.float32), document_index)
    readout = readout.reshape(TOKENS, GROUPS, STATE)
    summed = jnp.zeros((TOKENS, GROUPS, per_group, HEAD_DIM), jnp.float32)
    for sweep_direction in range(2):
        head_step_length = jax.nn.softplus(step_before_softplus.astype(jnp.float32) + head_step_bias[sweep_direction])
        decay_logarithm = -jnp.exp(head_rate_logarithm[sweep_direction]) * head_step_length + sudden_log_decay
        decay_logarithm = decay_logarithm.reshape(TOKENS, GROUPS, per_group)
        scaled = values * head_step_length.reshape(TOKENS, GROUPS, per_group)[..., None]
        arrays = (scaled, entries, readout, decay_logarithm, document_index)
        if sweep_direction == 1:
            arrays = tuple((jnp.flip(array, 0) for array in arrays))
        start_state = jnp.zeros((GROUPS, per_group, HEAD_DIM, STATE), jnp.float32)
        output, _ = sweep_blocks(*arrays, start_state, jnp.int32(-1), BLOCK)
        if sweep_direction == 1:
            output = jnp.flip(output, 0)
        summed = summed + output
    gated = summed.reshape(TOKENS, GROUPS, per_group * HEAD_DIM)
    gated = gated * jax.nn.silu(output_gate_rows.astype(jnp.float32)).reshape(TOKENS, GROUPS, per_group * HEAD_DIM)
    gated = gated * lax.rsqrt(lax.optimization_barrier(jnp.mean(gated * gated, axis=2, keepdims=True)) + norm_eps)
    normed = (gated.reshape(TOKENS, INNER) * group_norm_gain).astype(jnp.bfloat16)
    out_blocks = mixer_output_weight.astype(jnp.float32).reshape(N_TP, INNER // N_TP, D)
    down_blocks = down_projection_weight.astype(jnp.float32).reshape(D, N_TP, FF // N_TP)

    def dense_rows(pieces):
        normed_rows, stream_rows = pieces
        mixer_sum = block_sums(normed_rows.astype(jnp.float32).reshape(-1, N_TP, INNER // N_TP), out_blocks)
        first_sum = resid_scale * stream_rows.astype(jnp.float32) + mixer_sum
        normed_one = layer_norm(first_sum, mixer_norm_gain)
        hidden = jnp.dot(normed_one, up_projection_weight, preferred_element_type=jnp.float32)
        squared = jnp.square(jax.nn.relu(hidden)).astype(jnp.bfloat16)
        parts = jnp.einsum('tjf,djf->jtd', squared.astype(jnp.float32).reshape(-1, N_TP, FF // N_TP), down_blocks)
        rounded = lax.optimization_barrier(parts.astype(jnp.bfloat16))
        down_sum = lax.optimization_barrier(jnp.sum(rounded.astype(jnp.float32), axis=0))
        second_sum = resid_scale * normed_one.astype(jnp.float32) + down_sum
        return layer_norm(second_sum, channel_norm_gain)
    result = lax.map(dense_rows, (normed.reshape(N_SP, TOK_DEV, INNER), stream.reshape(N_SP, TOK_DEV, D)))
    return result.reshape(TOKENS, D)
```

```python
import jax
import jax.numpy as jnp
from jax import lax
from jax.experimental import pallas as pl
from jax.experimental.pallas import tpu as pltpu
from jax.sharding import PartitionSpec as P

HEAD_DIM = 64
STATE = 128
BLOCK = 128
LONGEST_DOCUMENT = 6144
PIECES = 2


exact_prec = lax.Precision.HIGHEST
norm_eps = 1e-05
resid_scale = 1.4142135623730951
bf16 = jnp.bfloat16
f32 = jnp.float32


def swap(array):
    return lax.ppermute(array, "tp", [(0, 1), (1, 0)])


def tp_scatter(partial):
    if lax.axis_size("tp") != 2:
        return lax.psum_scatter(
            partial.astype(bf16), "tp", scatter_dimension=1, tiled=True
        ).astype(f32)
    me = lax.axis_index("tp")
    width = partial.shape[1] // 2
    rounded = partial.astype(bf16)
    other = lax.dynamic_slice_in_dim(rounded, (1 - me) * width, width, 1)
    mine = lax.dynamic_slice_in_dim(rounded, me * width, width, 1)
    return mine.astype(f32) + swap(other).astype(f32)


def tp_gather(array):
    if lax.axis_size("tp") != 2:
        return lax.all_gather(array, "tp", axis=1, tiled=True)
    other = swap(array)
    first = lax.axis_index("tp") == 0
    return jnp.concatenate(
        [jnp.where(first, array, other), jnp.where(first, other, array)], axis=1
    )


def norm_rows(residual, gain, width):
    sums = jnp.stack([jnp.sum(residual, axis=1), jnp.sum(residual * residual, axis=1)])
    if lax.axis_size("tp") == 2:
        sums = sums + swap(sums)
    else:
        sums = lax.psum(sums, "tp")
    row_mean = sums[0] / width
    row_var = sums[1] / width - row_mean * row_mean
    return ((residual - row_mean[:, None]) * lax.rsqrt(row_var + norm_eps)[:, None] * gain).astype(
        bf16
    )


def pair_swap(array, bit=1):
    count = lax.axis_size("sp")
    return lax.ppermute(array, "sp", [(i, i ^ bit) for i in range(count)])


def pair_weights(weight):
    count = lax.axis_size("sp")
    odd = lax.axis_index("sp") % 2
    width = weight.shape[1] // 2
    mine = lax.dynamic_slice_in_dim(weight, odd * width, width, 1)
    other = pair_swap(lax.dynamic_slice_in_dim(weight, (1 - odd) * width, width, 1))
    both = jnp.concatenate(
        [jnp.where(odd == 0, mine, other), jnp.where(odd == 0, other, mine)], axis=0
    )
    members = [list(range(0, count, 2)), list(range(1, count, 2))]
    return lax.all_gather(both, "sp", axis=0, tiled=True, axis_index_groups=members)


def has_rings():
    return lax.axis_size("tp") == 2 and lax.axis_size("sp") == 4 * len(PAIR_STEPS)


def parity():
    return lax.axis_index("sp") % 2


def pair_order(count):
    depth = count // 4
    return [2 * z for z in range(depth)] + [2 * z + 1 for z in reversed(range(depth))]


def halves(weight):
    width = weight.shape[1] // 2
    mine = lax.dynamic_slice_in_dim(weight, parity() * width, width, 1)
    return mine, pair_swap(lax.dynamic_slice_in_dim(weight, (1 - parity()) * width, width, 1))


def ring_weights(weight):
    odd = lax.axis_index("sp") % 2
    mine, other = halves(weight)
    both = jnp.concatenate(
        [jnp.where(odd == 0, mine, other), jnp.where(odd == 0, other, mine)], axis=0
    )
    members = []
    for which in range(2):
        order = pair_order(lax.axis_size("sp"))
        members.append([2 * pair + which for pair in order])
    return lax.all_gather(both, "sp", axis=0, tiled=True, axis_index_groups=members)


MESH_ID = pl.DeviceIdType.MESH
PAIR_STEPS = ((2, 6), (5, 1), (3, 7), (0, 4))


def ring_place(spot, depth):
    far = spot // depth
    return spot + far * (2 * depth - 1 - 2 * spot), far


def mixer_kernel(
    rows_ref,
    mine_ref,
    other_ref,
    up_ref,
    sum_ref,
    down,
    up,
    rows,
    squared,
    local,
    send_t,
    recv_t,
    keep_x,
    send_x,
    recv_x,
    up_sem,
    own_sem,
    row_send,
    row_recv,
    ring_send,
    ring_recv,
    t_sems,
    x_sems,
):
    count = lax.axis_size("sp")
    depth = count // 4
    size = count // 2
    place = lax.axis_index("sp")
    me = lax.axis_index("tp")
    z, y, x = place // 4, (place // 2) % 2, place % 2
    spot = z + y * (2 * depth - 1 - 2 * z)
    height, width = rows_ref.shape
    half = height // 2
    full = 2 * width

    def member(where):
        level, far = ring_place(where, depth)
        return level * 4 + far * 2 + x

    after = (member((spot + 1) % size), me)
    before = (member((spot + size - 1) % size), me)
    across = place + 1 - 2 * x
    twin = (place, 1 - me)
    opposite = (across, me)

    barrier = pltpu.get_barrier_semaphore()
    near = (after, before, twin, opposite)
    for device in near:
        pl.semaphore_signal(barrier, inc=1, device_id=device, device_id_type=MESH_ID)
    pl.semaphore_wait(barrier, len(near))

    def remote(source, target, send, recv, device):
        return pltpu.make_async_remote_copy(
            src_ref=source,
            dst_ref=target,
            send_sem=send,
            recv_sem=recv,
            device_id=device,
            device_id_type=MESH_ID,
        )

    pending = []

    def ring(direction, distance, part, source):
        to = after if direction == 0 else before
        offset = (size - distance - 1) % size if direction == 0 else distance + 1
        n = 2 * distance + part
        copy = remote(
            source,
            down.at[2 * offset + part],
            ring_send.at[direction, n],
            ring_recv.at[direction, n],
            to,
        )
        copy.start()
        pending.append(copy)
        return copy

    last = size // 2 - 1
    flights = {}
    for direction in (0, 1):
        for part in (0, 1) if direction == 0 else (1, 0):
            flights[direction, 0, part] = ring(
                direction, 0, part, mine_ref if part == 0 else other_ref
            )

    def forward(distance, turn):
        for direction in (0, 1):
            part = turn if direction == 0 else 1 - turn
            flights[direction, distance - 1, part].wait_recv()
            if distance < last or (distance == last and turn == 0):
                offset = (size - distance) % size if direction == 0 else distance
                flights[direction, distance, part] = ring(
                    direction, distance, part, down.at[2 * offset + part]
                )

    my_columns = pl.ds(pl.multiple_of(me * width, width), width)
    parts = [pl.ds(i * half, half) for i in range(4)]
    to_twin = remote(
        rows_ref, rows.at[pl.ds(0, height), my_columns], row_send.at[0], row_recv.at[0], twin
    )
    outward = [
        remote(
            rows_ref.at[parts[i]],
            rows.at[parts[2 + i], my_columns],
            row_send.at[1 + i],
            row_recv.at[1 + i],
            opposite,
        )
        for i in range(2)
    ]
    inward = [
        remote(
            rows.at[parts[2 + i], my_columns],
            rows.at[parts[2 + i], my_columns],
            row_send.at[3 + i],
            row_recv.at[3 + i],
            twin,
        )
        for i in range(2)
    ]
    for copy in [to_twin] + outward:
        copy.start()
    pending.extend([to_twin] + outward + inward)

    order = pair_order(count)
    step = 2 * (full // count)
    loads = [
        pltpu.make_async_copy(
            up_ref.at[pl.ds(i * step, step)], up.at[pl.ds(q * step, step)], up_sem.at[i]
        )
        for i, q in enumerate(order)
    ]
    own = [
        pltpu.make_async_copy(mine_ref, down.at[0], own_sem.at[0]),
        pltpu.make_async_copy(other_ref, down.at[1], own_sem.at[1]),
    ]
    for copy in loads + own:
        copy.start()
    rows[pl.ds(0, height), my_columns] = rows_ref[...]
    to_twin.wait_recv()
    for copy in loads:
        copy.wait()

    hidden_width = up.shape[1]
    tile = 2 * down.shape[1]

    def raise_rows(start, length):
        def body(i, carry):
            columns = pl.ds(pl.multiple_of(i * tile, tile), tile)
            value = jnp.dot(
                rows[pl.ds(start, length), :], up[:, columns], preferred_element_type=f32
            )
            value = jnp.maximum(value, 0.0)
            squared[pl.ds(start, length), columns] = (value * value).astype(bf16)
            return carry

        lax.fori_loop(0, hidden_width // tile, body, 0)

    raise_rows(0, height)
    forward(1, 0)
    outward[0].wait_recv()
    inward[0].start()
    forward(1, 1)
    inward[0].wait_recv()
    raise_rows(height, half)
    forward(2, 0)
    outward[1].wait_recv()
    inward[1].start()
    inward[1].wait_recv()
    raise_rows(height + half, half)
    forward(2, 1)
    for copy in own:
        copy.wait()

    def owner(where):
        level, _ = ring_place(where, depth)
        return level // (depth // 2)

    def product(slot, start, length):
        weights = down[pl.ds(2 * slot, 2)].reshape(tile, hidden_width)
        return lax.dot_general(
            squared[pl.ds(start, length), :],
            weights,
            (((1,), (1,)), ((), ())),
            preferred_element_type=f32,
        )

    handed, returned = [], []

    def lower(j):
        first, second = PAIR_STEPS[j]
        ours = (owner((spot + first) % size) + me + 1) % 2
        kept = second + (first - second) * ours
        given = first + second - kept
        for i in (2, 3, 0, 1):
            send_t[j, parts[i]] = product(given, i * half, half).astype(bf16)
        copy = remote(send_t.at[j], recv_t.at[j], t_sems.at[0, j], t_sems.at[1, j], twin)
        copy.start()
        handed.append(copy)
        pending.append(copy)
        for i in (0, 1):
            keep_x[j, parts[i]] = product(kept, height + i * half, half)
        for i in (0, 1):
            local[j, parts[i]] = product(kept, i * half, half)
        copy.wait_recv()
        send_x[j] = (keep_x[j] + recv_t[j, pl.ds(height, height)].astype(f32)).astype(bf16)
        copy = remote(send_x.at[j], recv_x.at[j], x_sems.at[0, j], x_sems.at[1, j], opposite)
        copy.start()
        returned.append(copy)
        pending.append(copy)

    piece = tile // 2

    sum_ref[...] = resid_scale * rows_ref[...].astype(f32)

    def settle(j):
        first, second = PAIR_STEPS[j]
        at_first = (spot + first) % size
        at_second = (spot + second) % size
        ours = (owner(at_first) + me + 1) % 2
        source = member(at_second + (at_first - at_second) * ours)
        base = source - me * (count // 2)
        pair = base + 1 - 2 * (source % 2)
        returned[j].wait_recv()
        for part, spot_at in enumerate((base, pair)):
            columns = pl.ds(part * piece, piece)
            swapped = pl.ds((1 - part) * piece, piece)
            target = pl.ds(pl.multiple_of(spot_at * piece, piece), piece)
            sum_ref[:, target] += (
                local[j, :, columns]
                + recv_t[j, pl.ds(0, height), columns].astype(f32)
                + recv_x[j, :, swapped].astype(f32)
            )

    lower(0)
    forward(3, 0)
    forward(3, 1)
    lower(1)
    settle(0)
    lower(2)
    settle(1)
    forward(4, 0)
    lower(3)
    settle(2)
    settle(3)
    for copy in pending:
        copy.wait_send()


def ring_mixer(rows, mine, other, up_half):
    count = lax.axis_size("sp")
    height, width = rows.shape
    tile, steps, size = 2 * mine.shape[0], len(PAIR_STEPS), count // 2
    piece, hidden = mine.shape
    dma = pltpu.SemaphoreType.DMA
    vmem, anywhere = pl.BlockSpec(memory_space=pltpu.VMEM), pl.BlockSpec(memory_space=pl.ANY)
    return pl.pallas_call(
        mixer_kernel,
        out_shape=jax.ShapeDtypeStruct((height, width), f32),
        in_specs=[vmem, anywhere, anywhere, anywhere],
        out_specs=vmem,
        scratch_shapes=[
            pltpu.VMEM((count, piece, hidden), bf16),
            pltpu.VMEM((2 * width, hidden), bf16),
            pltpu.VMEM((2 * height, 2 * width), bf16),
            pltpu.VMEM((2 * height, hidden), bf16),
            pltpu.VMEM((steps, height, tile), f32),
            pltpu.VMEM((steps, 2 * height, tile), bf16),
            pltpu.VMEM((steps, 2 * height, tile), bf16),
            pltpu.VMEM((steps, height, tile), f32),
            pltpu.VMEM((steps, height, tile), bf16),
            pltpu.VMEM((steps, height, tile), bf16),
            dma((size,)),
            dma((2,)),
            dma((5,)),
            dma((5,)),
            dma((2, size)),
            dma((2, size)),
            dma((2, steps)),
            dma((2, steps)),
        ],
        compiler_params=pltpu.CompilerParams(
            collective_id=0, has_side_effects=True, vmem_limit_bytes=60 * 1024 * 1024
        ),
        cost_estimate=pl.CostEstimate(
            flops=8 * height * 2 * width * hidden, bytes_accessed=30000000, transcendentals=0
        ),
    )(rows, mine, other, up_half)


def channel_mixer(rows, up, down):
    hidden = jnp.dot(tp_gather(rows), up, preferred_element_type=f32)
    squared = jnp.square(jax.nn.relu(hidden)).astype(bf16)
    part = lax.dot_general(squared, down, (((1,), (1,)), ((), ())), preferred_element_type=f32)
    return tp_scatter(part)


def shifted(array, step):
    count = lax.axis_size("sp")
    if step > 0:
        pairs = [(i, i + step) for i in range(count - step)]
    else:
        pairs = [(i, i + step) for i in range(-step, count)]
    return lax.ppermute(array, "sp", pairs)


def with_decay(state, through):
    heads = through.size
    flat = state.reshape(heads, -1).astype(bf16)
    through = through.reshape(heads, 1)
    high = through.astype(bf16)
    middle = (through - high.astype(f32)).astype(bf16)
    low = (through - high.astype(f32) - middle.astype(f32)).astype(bf16)
    terms = jnp.concatenate([high, middle, low], axis=1)
    return jnp.concatenate([flat, jnp.pad(terms, ((0, 0), (0, 125)))], axis=1)


def apart(packed, shape):
    terms = packed[:, -128:].astype(f32)
    through = terms[:, 0] + (terms[:, 1] + terms[:, 2])
    return packed[:, :-128].astype(f32).reshape(shape), through.reshape(shape[:2])


def incoming_state(end_state, own_pass, direction, reach):
    count = lax.axis_size("sp")
    shape = end_state.shape
    state, through = apart(shifted(with_decay(end_state, own_pass), direction), shape)
    covered = 1
    while covered < min(reach, count - 1):
        more, further = apart(shifted(with_decay(state, through), direction * covered), shape)
        state = state + through[..., None, None] * more
        through = through * further
        covered *= 2
    return state


def per_device(
    head_value_rows,
    entry_map_rows,
    readout_map_rows,
    output_gate_rows,
    step_before_softplus,
    sudden_log_decay,
    document_index,
    head_rate_logarithm,
    head_step_bias,
    value_conv_taps,
    entry_conv_taps,
    readout_conv_taps,
    group_norm_gain,
    mixer_output_weight,
    stream,
    mixer_norm_gain,
    channel_norm_gain,
    up_projection_weight,
    down_projection_weight,
):
    if has_rings():
        up_half = ring_weights(up_projection_weight)
        mine, other = halves(down_projection_weight)
    else:
        up_half = pair_weights(up_projection_weight)
        down_half = pair_weights(down_projection_weight)

    rows = head_value_rows.shape[0]
    heads = step_before_softplus.shape[1]
    groups = entry_map_rows.shape[1] // STATE
    per_group = heads // groups
    value_width = head_value_rows.shape[1]
    state_width = entry_map_rows.shape[1]
    model_width = mixer_output_weight.shape[1]
    blocks = rows // BLOCK
    sp_count = lax.axis_size("sp")
    place = lax.axis_index("sp")
    position = place * rows

    taps = value_conv_taps.shape[0]
    half = taps // 2
    ends = jnp.concatenate(
        [
            jnp.concatenate([a[rows - half :], a[:half]], axis=0)
            for a in (head_value_rows, entry_map_rows, readout_map_rows)
        ],
        axis=1,
    )
    low_all = shifted(ends[:half], 1)
    high_all = shifted(ends[half:], -1)
    doc_pad = jnp.pad(document_index, half + 1, constant_values=-1)
    window_ids = lax.dynamic_slice_in_dim(doc_pad, position + 1, rows + 2 * half)
    own_ids = window_ids[half : half + rows]
    prev_id = window_ids[half - 1]
    next_id = window_ids[half + rows]

    def conv(array, weights, start):
        width = array.shape[1]
        extended = jnp.concatenate(
            [low_all[:, start : start + width], array, high_all[:, start : start + width]], axis=0
        )
        weights = weights.astype(f32)
        total = weights[half] * array.astype(f32)
        for offset in range(taps):
            if offset == half:
                continue
            same = (window_ids[offset : offset + rows] == own_ids)[:, None]
            total = total + weights[offset] * jnp.where(
                same, extended[offset : offset + rows].astype(f32), 0.0
            )
        return jax.nn.silu(total).astype(bf16)

    values = conv(head_value_rows, value_conv_taps, 0)
    entries = conv(entry_map_rows, entry_conv_taps, value_width)
    readout = conv(readout_map_rows, readout_conv_taps, value_width + state_width)
    values = values.reshape(blocks, BLOCK, groups, per_group, HEAD_DIM)
    entries = entries.reshape(blocks, BLOCK, groups, STATE)
    readout = readout.reshape(blocks, BLOCK, groups, STATE)

    raw = step_before_softplus.astype(f32).T
    steps = jax.nn.softplus(raw[None] + head_step_bias[:, :, None])
    decay = -jnp.exp(head_rate_logarithm)[:, :, None] * steps + sudden_log_decay.T[None]
    shape = (2, groups, per_group, blocks, BLOCK)
    steps = jnp.transpose(steps.reshape(shape), (0, 3, 1, 2, 4))
    decay = jnp.transpose(decay.reshape(shape), (0, 3, 1, 2, 4))
    at = lax.iota(jnp.int32, BLOCK)
    upto = (at[:, None] <= at[None, :]).astype(f32)
    running = jnp.einsum("kbgrs,st->kbgrt", decay, upto, precision=exact_prec)
    totals = running[..., -1]
    ahead = running[0]
    behind = running[1] - decay[1]

    ids = own_ids.reshape(blocks, BLOCK)
    first_ids, last_ids = ids[:, 0], ids[:, -1]
    before = jnp.concatenate([prev_id[None], last_ids[:-1]])
    after = jnp.concatenate([first_ids[1:], next_id[None]])
    pass_f = jnp.where((before == last_ids)[:, None, None], jnp.exp(totals[0]), 0.0)
    pass_b = jnp.where((after == first_ids)[:, None, None], jnp.exp(totals[1]), 0.0)
    end_f = jnp.where(
        (ids == last_ids[:, None])[:, None, None], jnp.exp(totals[0][..., None] - ahead), 0.0
    ) * steps[0]
    end_b = jnp.where((ids == first_ids[:, None])[:, None, None], jnp.exp(behind), 0.0) * steps[1]
    arrive_f = jnp.where((ids == before[:, None])[:, None, None], jnp.exp(ahead), 0.0)
    arrive_b = jnp.where(
        (ids == after[:, None])[:, None, None], jnp.exp(totals[1][..., None] - behind), 0.0
    )

    own_f, own_b = jnp.prod(pass_f, axis=0), jnp.prod(pass_b, axis=0)

    def fresh_states(weight):
        weighted = values.astype(f32) * jnp.transpose(weight, (0, 3, 1, 2))[..., None]
        return jnp.einsum(
            "bsgrp,bsgn->bgrpn", weighted.astype(bf16), entries, preferred_element_type=f32
        )

    fresh_f = fresh_states(end_f)
    fresh_b = fresh_states(end_b)

    end_state = fresh_f[0]
    for b in range(1, blocks):
        end_state = end_state * pass_f[b][..., None, None] + fresh_f[b]
    start_state = fresh_b[blocks - 1]
    for b in range(blocks - 2, -1, -1):
        start_state = start_state * pass_b[b][..., None, None] + fresh_b[b]
    reach = -(-LONGEST_DOCUMENT // rows)
    in_f = incoming_state(end_state, own_f, 1, reach)
    in_b = incoming_state(start_state, own_b, -1, reach)

    scores = jnp.einsum("btgn,bsgn->bgts", readout, entries, preferred_element_type=f32)
    later = at[:, None] > at[None, :]
    equal = at[:, None] == at[None, :]
    linked = (ids[:, :, None] == ids[:, None, :])[:, None, None]
    spread = jnp.where(
        later,
        ahead[..., :, None] - ahead[..., None, :],
        behind[..., None, :] - behind[..., :, None],
    )
    strength = jnp.where(
        later,
        steps[0][..., None, :],
        jnp.where(equal, steps[0][..., None, :], 0.0) + steps[1][..., None, :],
    )
    weights = jnp.where(linked, jnp.exp(spread) * strength, 0.0)
    mixing = (scores[:, :, None] * weights).astype(bf16)
    output = jnp.einsum("bgrts,bsgrp->bgrtp", mixing, values, preferred_element_type=f32)

    state_f = [in_f]
    for b in range(blocks - 1):
        state_f.append(state_f[-1] * pass_f[b][..., None, None] + fresh_f[b])
    state_b = [in_b]
    for b in range(blocks - 1, 0, -1):
        state_b.append(state_b[-1] * pass_b[b][..., None, None] + fresh_b[b])
    entering_f = jnp.stack([s.astype(bf16) for s in state_f])
    entering_b = jnp.stack([s.astype(bf16) for s in state_b[::-1]])
    carried_f = jnp.einsum("btgn,bgrpn->bgrtp", readout, entering_f, preferred_element_type=f32)
    carried_b = jnp.einsum("btgn,bgrpn->bgrtp", readout, entering_b, preferred_element_type=f32)
    output = output + carried_f * arrive_f[..., None] + carried_b * arrive_b[..., None]

    gated = jnp.transpose(output, (0, 3, 1, 2, 4)).reshape(rows, groups, per_group * HEAD_DIM)
    gated = gated * jax.nn.silu(output_gate_rows.astype(f32)).reshape(gated.shape)
    gated = gated * lax.rsqrt(jnp.mean(gated * gated, axis=2, keepdims=True) + norm_eps)
    normed = (gated.reshape(rows, value_width) * group_norm_gain).astype(bf16)

    mixer_sum = tp_scatter(jnp.dot(normed, mixer_output_weight, preferred_element_type=f32))
    first_sum = resid_scale * stream.astype(f32) + mixer_sum
    normed_one = norm_rows(first_sum, mixer_norm_gain, model_width)
    if has_rings():
        second_sum = ring_mixer(normed_one, mine, other, up_half)
        return norm_rows(second_sum, channel_norm_gain, model_width)
    piece = rows // PIECES
    returned = [
        pair_swap(
            channel_mixer(
                pair_swap(normed_one[i * piece : (i + 1) * piece]),
                up_half,
                down_half,
            ).astype(bf16)
        )
        for i in range(PIECES)
    ]
    down_sum = channel_mixer(normed_one, up_half, down_half) + jnp.concatenate(returned).astype(f32)
    second_sum = resid_scale * normed_one.astype(f32) + down_sum
    return norm_rows(second_sum, channel_norm_gain, model_width)


def solution(mesh):
    placed = (
        P("sp", "tp"),
        P("sp", "tp"),
        P("sp", "tp"),
        P("sp", "tp"),
        P("sp", "tp"),
        P("sp", "tp"),
        P(),
        P(None, "tp"),
        P(None, "tp"),
        P(None, "tp"),
        P(None, "tp"),
        P(None, "tp"),
        P("tp"),
        P("tp", None),
        P("sp", "tp"),
        P("tp"),
        P("tp"),
        P("sp", "tp"),
        P("sp", "tp"),
    )
    return jax.shard_map(
        per_device, mesh=mesh, in_specs=placed, out_specs=P("sp", "tp"), check_vma=False
    )
```

```python
import jax
import jax.numpy as jnp
from jax import lax
from jax.experimental import pallas as pl
from jax.experimental.pallas import tpu as pltpu
from jax.sharding import PartitionSpec as P

HEAD_DIM = 64
STATE = 128
BLOCK = 128
LONGEST_DOCUMENT = 6144
PIECES = 2


exact_prec = lax.Precision.HIGHEST
norm_eps = 1e-05
resid_scale = 1.4142135623730951
bf16 = jnp.bfloat16
f32 = jnp.float32


def swap(array):
    return lax.ppermute(array, "tp", [(0, 1), (1, 0)])


def tp_scatter(partial):
    if lax.axis_size("tp") != 2:
        return lax.psum_scatter(
            partial.astype(bf16), "tp", scatter_dimension=1, tiled=True
        ).astype(f32)
    me = lax.axis_index("tp")
    width = partial.shape[1] // 2
    rounded = partial.astype(bf16)
    other = lax.dynamic_slice_in_dim(rounded, (1 - me) * width, width, 1)
    mine = lax.dynamic_slice_in_dim(rounded, me * width, width, 1)
    return mine.astype(f32) + swap(other).astype(f32)


def tp_gather(array):
    if lax.axis_size("tp") != 2:
        return lax.all_gather(array, "tp", axis=1, tiled=True)
    other = swap(array)
    first = lax.axis_index("tp") == 0
    return jnp.concatenate(
        [jnp.where(first, array, other), jnp.where(first, other, array)], axis=1
    )


def norm_rows(residual, gain, width):
    sums = jnp.stack([jnp.sum(residual, axis=1), jnp.sum(residual * residual, axis=1)])
    if lax.axis_size("tp") == 2:
        sums = sums + swap(sums)
    else:
        sums = lax.psum(sums, "tp")
    row_mean = sums[0] / width
    row_var = sums[1] / width - row_mean * row_mean
    return ((residual - row_mean[:, None]) * lax.rsqrt(row_var + norm_eps)[:, None] * gain).astype(
        bf16
    )


def pair_swap(array, bit=1):
    count = lax.axis_size("sp")
    return lax.ppermute(array, "sp", [(i, i ^ bit) for i in range(count)])


def pair_weights(weight):
    count = lax.axis_size("sp")
    odd = lax.axis_index("sp") % 2
    width = weight.shape[1] // 2
    mine = lax.dynamic_slice_in_dim(weight, odd * width, width, 1)
    other = pair_swap(lax.dynamic_slice_in_dim(weight, (1 - odd) * width, width, 1))
    both = jnp.concatenate(
        [jnp.where(odd == 0, mine, other), jnp.where(odd == 0, other, mine)], axis=0
    )
    members = [list(range(0, count, 2)), list(range(1, count, 2))]
    return lax.all_gather(both, "sp", axis=0, tiled=True, axis_index_groups=members)


def has_rings():
    return lax.axis_size("tp") == 2 and lax.axis_size("sp") == 2 * RING


def parity():
    return lax.axis_index("sp") % 2


def pair_order(count):
    depth = count // 4
    return [2 * z for z in range(depth)] + [2 * z + 1 for z in reversed(range(depth))]


def halves(weight):
    width = weight.shape[1] // 2
    mine = lax.dynamic_slice_in_dim(weight, parity() * width, width, 1)
    return mine, pair_swap(lax.dynamic_slice_in_dim(weight, (1 - parity()) * width, width, 1))


def ring_weights(weight):
    odd = lax.axis_index("sp") % 2
    mine, other = halves(weight)
    both = jnp.concatenate(
        [jnp.where(odd == 0, mine, other), jnp.where(odd == 0, other, mine)], axis=0
    )
    members = []
    for which in range(2):
        order = pair_order(lax.axis_size("sp"))
        members.append([2 * pair + which for pair in order])
    return lax.all_gather(both, "sp", axis=0, tiled=True, axis_index_groups=members)


MESH_ID = pl.DeviceIdType.MESH
RING = 8


def ring_place(spot, depth):
    far = spot // depth
    return spot + far * (2 * depth - 1 - 2 * spot), far


def mixer_kernel(
    rows_ref,
    mine_ref,
    other_ref,
    up_ref,
    sum_ref,
    down,
    up,
    rows,
    squared,
    local,
    send_t,
    recv_t,
    keep_x,
    send_x,
    recv_x,
    up_sem,
    own_sem,
    row_send,
    row_recv,
    ring_send,
    ring_recv,
    t_sems,
    x_sems,
):
    count = lax.axis_size("sp")
    depth = count // 4
    size = count // 2
    place = lax.axis_index("sp")
    me = lax.axis_index("tp")
    z, y, x = place // 4, (place // 2) % 2, place % 2
    spot = z + y * (2 * depth - 1 - 2 * z)
    height, width = rows_ref.shape
    half = height // 2
    full = 2 * width

    def member(where):
        level, far = ring_place(where, depth)
        return level * 4 + far * 2 + x

    after = (member((spot + 1) % size), me)
    before = (member((spot + size - 1) % size), me)
    across = place + 1 - 2 * x
    twin = (place, 1 - me)
    opposite = (across, me)

    barrier = pltpu.get_barrier_semaphore()
    near = (after, before, twin, opposite)
    for device in near:
        pl.semaphore_signal(barrier, inc=1, device_id=device, device_id_type=MESH_ID)
    pl.semaphore_wait(barrier, len(near))

    def remote(source, target, send, recv, device):
        return pltpu.make_async_remote_copy(
            src_ref=source,
            dst_ref=target,
            send_sem=send,
            recv_sem=recv,
            device_id=device,
            device_id_type=MESH_ID,
        )

    pending = []

    def ring(direction, distance, part, source):
        to = after if direction == 0 else before
        offset = (size - distance - 1) % size if direction == 0 else distance + 1
        n = 2 * distance + part
        copy = remote(
            source,
            down.at[2 * offset + part],
            ring_send.at[direction, n],
            ring_recv.at[direction, n],
            to,
        )
        copy.start()
        pending.append(copy)
        return copy

    last = size // 2 - 1
    flights = {}
    for direction in (0, 1):
        for part in (0, 1) if direction == 0 else (1, 0):
            flights[direction, 0, part] = ring(
                direction, 0, part, mine_ref if part == 0 else other_ref
            )

    def forward(distance, turn):
        for direction in (0, 1):
            part = turn if direction == 0 else 1 - turn
            flights[direction, distance - 1, part].wait_recv()
            if distance < last or (distance == last and turn == 0):
                offset = (size - distance) % size if direction == 0 else distance
                flights[direction, distance, part] = ring(
                    direction, distance, part, down.at[2 * offset + part]
                )

    my_columns = pl.ds(pl.multiple_of(me * width, width), width)
    parts = [pl.ds(i * half, half) for i in range(4)]
    to_twin = remote(
        rows_ref, rows.at[pl.ds(0, height), my_columns], row_send.at[0], row_recv.at[0], twin
    )
    outward = [
        remote(
            rows_ref.at[parts[i]],
            rows.at[parts[2 + i], my_columns],
            row_send.at[1 + i],
            row_recv.at[1 + i],
            opposite,
        )
        for i in range(2)
    ]
    inward = [
        remote(
            rows.at[parts[2 + i], my_columns],
            rows.at[parts[2 + i], my_columns],
            row_send.at[3 + i],
            row_recv.at[3 + i],
            twin,
        )
        for i in range(2)
    ]
    for copy in [to_twin] + outward:
        copy.start()
    pending.extend([to_twin] + outward + inward)

    order = pair_order(count)
    step = 2 * (full // count)
    loads = [
        pltpu.make_async_copy(
            up_ref.at[pl.ds(i * step, step)], up.at[pl.ds(q * step, step)], up_sem.at[i]
        )
        for i, q in enumerate(order)
    ]
    own = [
        pltpu.make_async_copy(mine_ref, down.at[0], own_sem.at[0]),
        pltpu.make_async_copy(other_ref, down.at[1], own_sem.at[1]),
    ]
    for copy in loads + own:
        copy.start()
    rows[pl.ds(0, height), my_columns] = rows_ref[...]
    to_twin.wait_recv()
    for copy in loads:
        copy.wait()

    hidden_width = up.shape[1]
    tile = 2 * down.shape[1]

    def raise_rows(start, length):
        def body(i, carry):
            columns = pl.ds(pl.multiple_of(i * tile, tile), tile)
            value = jnp.dot(
                rows[pl.ds(start, length), :], up[:, columns], preferred_element_type=f32
            )
            value = jnp.maximum(value, 0.0)
            squared[pl.ds(start, length), columns] = (value * value).astype(bf16)
            return carry

        lax.fori_loop(0, hidden_width // tile, body, 0)

    raise_rows(0, height)
    forward(1, 0)
    outward[0].wait_recv()
    inward[0].start()
    forward(1, 1)
    inward[0].wait_recv()
    raise_rows(height, half)
    forward(2, 0)
    outward[1].wait_recv()
    inward[1].start()
    inward[1].wait_recv()
    raise_rows(height + half, half)
    for copy in own:
        copy.wait()

    def owner(where):
        level, _ = ring_place(where, depth)
        return level // (depth // 2)

    def product(slot, start):
        return lax.dot_general(
            squared[pl.ds(start, height), :],
            down[pl.ds(2 * slot, 2)].reshape(tile, hidden_width),
            (((1,), (1,)), ((), ())),
            preferred_element_type=f32,
        )

    own_rows, far_rows = pl.ds(0, height), pl.ds(height, height)
    handed = [
        remote(send_t.at[i], recv_t.at[i], t_sems.at[0, i], t_sems.at[1, i], twin)
        for i in range(2 * size)
    ]
    returned = [
        remote(send_x.at[i], recv_x.at[i], x_sems.at[0, i], x_sems.at[1, i], opposite)
        for i in range(size)
    ]
    is_ours = [owner((spot + i) % size) == me for i in range(size)]
    is_theirs = [owner((spot + i) % size) != me for i in range(size)]

    def lower(i):
        keep_x[...] = product(i, height)

        @pl.when(is_theirs[i])
        def _():
            send_t[2 * i] = keep_x[...].astype(bf16)
            handed[2 * i].start()

        local[i] = product(i, 0).astype(bf16)

        @pl.when(is_ours[i])
        def _():
            handed[2 * i].wait_recv()
            send_x[i] = (keep_x[...] + recv_t[2 * i].astype(f32)).astype(bf16)
            returned[i].start()

        @pl.when(is_theirs[i])
        def _():
            send_t[2 * i + 1] = local[i]
            handed[2 * i + 1].start()

    piece = tile // 2

    sum_ref[...] = resid_scale * rows_ref[...].astype(f32)

    def settle(i):
        @pl.when(is_ours[i])
        def _():
            base = member((spot + i) % size) - me * (count // 2)
            pair = base + 1 - 2 * x
            handed[2 * i + 1].wait_recv()
            returned[i].wait_recv()
            for part, spot_at in enumerate((base, pair)):
                columns = pl.ds(part * piece, piece)
                swapped = pl.ds((1 - part) * piece, piece)
                target = pl.ds(pl.multiple_of(spot_at * piece, piece), piece)
                sum_ref[:, target] += (
                    local[i, :, columns].astype(f32)
                    + recv_t[2 * i + 1, :, columns].astype(f32)
                    + recv_x[i, :, swapped].astype(f32)
                )

    lower(0)
    lower(1)
    lower(size - 1)
    forward(2, 1)
    lower(2)
    lower(size - 2)
    forward(3, 0)
    settle(0)
    settle(1)
    settle(size - 1)
    forward(3, 1)
    lower(3)
    lower(size - 3)
    settle(2)
    settle(size - 2)
    forward(4, 0)
    lower(4)
    settle(3)
    settle(size - 3)
    settle(4)
    for copy in pending:
        copy.wait_send()
    for i in range(size):

        @pl.when(is_theirs[i])
        def _(i=i):
            handed[2 * i].wait_send()
            handed[2 * i + 1].wait_send()

        @pl.when(is_ours[i])
        def _(i=i):
            returned[i].wait_send()


def ring_mixer(rows, mine, other, up_half):
    count = lax.axis_size("sp")
    height, width = rows.shape
    tile, size = 2 * mine.shape[0], count // 2
    piece, hidden = mine.shape
    dma = pltpu.SemaphoreType.DMA
    vmem, anywhere = pl.BlockSpec(memory_space=pltpu.VMEM), pl.BlockSpec(memory_space=pl.ANY)
    return pl.pallas_call(
        mixer_kernel,
        out_shape=jax.ShapeDtypeStruct((height, width), f32),
        in_specs=[vmem, anywhere, anywhere, anywhere],
        out_specs=vmem,
        scratch_shapes=[
            pltpu.VMEM((count, piece, hidden), bf16),
            pltpu.VMEM((2 * width, hidden), bf16),
            pltpu.VMEM((2 * height, 2 * width), bf16),
            pltpu.VMEM((2 * height, hidden), bf16),
            pltpu.VMEM((size, height, tile), bf16),
            pltpu.VMEM((2 * size, height, tile), bf16),
            pltpu.VMEM((2 * size, height, tile), bf16),
            pltpu.VMEM((height, tile), f32),
            pltpu.VMEM((size, height, tile), bf16),
            pltpu.VMEM((size, height, tile), bf16),
            dma((size,)),
            dma((2,)),
            dma((5,)),
            dma((5,)),
            dma((2, size)),
            dma((2, size)),
            dma((2, 2 * size)),
            dma((2, size)),
        ],
        compiler_params=pltpu.CompilerParams(
            collective_id=0, has_side_effects=True, vmem_limit_bytes=60 * 1024 * 1024
        ),
        cost_estimate=pl.CostEstimate(
            flops=8 * height * 2 * width * hidden, bytes_accessed=30000000, transcendentals=0
        ),
    )(rows, mine, other, up_half)


def channel_mixer(rows, up, down):
    hidden = jnp.dot(tp_gather(rows), up, preferred_element_type=f32)
    squared = jnp.square(jax.nn.relu(hidden)).astype(bf16)
    part = lax.dot_general(squared, down, (((1,), (1,)), ((), ())), preferred_element_type=f32)
    return tp_scatter(part)


def shifted(array, step):
    count = lax.axis_size("sp")
    if step > 0:
        pairs = [(i, i + step) for i in range(count - step)]
    else:
        pairs = [(i, i + step) for i in range(-step, count)]
    return lax.ppermute(array, "sp", pairs)


def with_decay(state, through):
    heads = through.size
    flat = state.reshape(heads, -1).astype(bf16)
    through = through.reshape(heads, 1)
    high = through.astype(bf16)
    middle = (through - high.astype(f32)).astype(bf16)
    low = (through - high.astype(f32) - middle.astype(f32)).astype(bf16)
    terms = jnp.concatenate([high, middle, low], axis=1)
    return jnp.concatenate([flat, jnp.pad(terms, ((0, 0), (0, 125)))], axis=1)


def apart(packed, shape):
    terms = packed[:, -128:].astype(f32)
    through = terms[:, 0] + (terms[:, 1] + terms[:, 2])
    return packed[:, :-128].astype(f32).reshape(shape), through.reshape(shape[:2])


def incoming_state(end_state, own_pass, direction, reach):
    count = lax.axis_size("sp")
    shape = end_state.shape
    state, through = apart(shifted(with_decay(end_state, own_pass), direction), shape)
    covered = 1
    while covered < min(reach, count - 1):
        more, further = apart(shifted(with_decay(state, through), direction * covered), shape)
        state = state + through[..., None, None] * more
        through = through * further
        covered *= 2
    return state


def scaled(state, scale, heads):
    head_dim = state.shape[0] // heads
    return jnp.concatenate(
        [
            state[h * head_dim : (h + 1) * head_dim] * scale[h : h + 1, :]
            for h in range(heads)
        ],
        axis=0,
    )


def spread_heads(columns, first, heads, lane):
    parts = []
    for h in range(0, heads, 2):
        parts.append(
            jnp.where(
                lane, columns[:, first + h : first + h + 1], columns[:, first + h + 1 : first + h + 2]
            )
        )
    return jnp.concatenate(parts, axis=1)


def states_kernel(
    value_ref,
    entry_ref,
    read_ref,
    gate_ref,
    steps_ref,
    decay_ref,
    edges_ref,
    ids_ref,
    same_ref,
    value_taps,
    entry_taps,
    read_taps,
    gain_ref,
    down_ref,
    out_ref,
    other_ref,
    ext,
    value_low,
    entry_low,
    read_low,
    value_high,
    entry_high,
    read_high,
    values,
    entries,
    reads,
    fresh,
    vectors,
    columns,
    passing,
    within,
    entering,
    send_a,
    decay_a,
    recv_a,
    table_a,
    send_b,
    decay_b,
    recv_b,
    table_b,
    send_c,
    recv_c,
    halo_sems,
    a_sems,
    b_sems,
    c_sems,
    swap_sems,
):
    count = lax.axis_size("sp")
    place = lax.axis_index("sp")
    me = lax.axis_index("tp")
    depth = count // 4
    z, q = place // 4, place % 4
    height = value_ref.shape[0]
    groups = steps_ref.shape[0]
    blocks = height // BLOCK
    heads = steps_ref.shape[1] // 2
    wide = heads * HEAD_DIM
    edge = value_low.shape[0]

    plane = [(z * 4 + (q + i) % 4, me) for i in (1, 2, 3)]
    tower = [(((z + i) % depth) * 4 + q, me) for i in range(1, depth)]
    up_place, down_place = (place + 1, me), (place - 1, me)

    barrier = pltpu.get_barrier_semaphore()

    @pl.when(place + 1 < count)
    def _():
        pl.semaphore_signal(barrier, inc=1, device_id=up_place, device_id_type=MESH_ID)

    @pl.when(place > 0)
    def _():
        pl.semaphore_signal(barrier, inc=1, device_id=down_place, device_id_type=MESH_ID)

    for device in plane + tower:
        pl.semaphore_signal(barrier, inc=1, device_id=device, device_id_type=MESH_ID)

    @pl.when((place > 0) & (place + 1 < count))
    def _():
        pl.semaphore_wait(barrier, len(plane) + len(tower) + 2)

    @pl.when((place == 0) | (place + 1 == count))
    def _():
        pl.semaphore_wait(barrier, len(plane) + len(tower) + 1)

    def remote(source, target, send, recv, device):
        return pltpu.make_async_remote_copy(
            src_ref=source,
            dst_ref=target,
            send_sem=send,
            recv_sem=recv,
            device_id=device,
            device_id_type=MESH_ID,
        )

    raw = (value_ref, entry_ref, read_ref)
    lows, highs = (value_low, entry_low, read_low), (value_high, entry_high, read_high)
    upward = [
        remote(
            raw[i].at[pl.ds(height - edge, edge)],
            lows[i],
            halo_sems.at[0, i],
            halo_sems.at[1, i],
            up_place,
        )
        for i in range(3)
    ]
    downward = [
        remote(
            raw[i].at[pl.ds(0, edge)], highs[i], halo_sems.at[2, i], halo_sems.at[3, i], down_place
        )
        for i in range(3)
    ]

    @pl.when(place + 1 < count)
    def _():
        for copy in upward:
            copy.start()

    @pl.when(place > 0)
    def _():
        for copy in downward:
            copy.start()

    x = place % 2
    share = other_ref.shape[1]
    swap_down = remote(
        down_ref.at[:, pl.ds(pl.multiple_of((1 - x) * share, share), share)],
        other_ref,
        swap_sems.at[0],
        swap_sems.at[1],
        (place + 1 - 2 * x, me),
    )
    swap_down.start()

    @pl.when(place == 0)
    def _():
        for low in lows:
            low[...] = jnp.zeros_like(low)

    @pl.when(place + 1 == count)
    def _():
        for high in highs:
            high[...] = jnp.zeros_like(high)

    @pl.when(place > 0)
    def _():
        for copy in upward:
            copy.wait_recv()

    @pl.when(place + 1 < count)
    def _():
        for copy in downward:
            copy.wait_recv()

    row_at = lax.broadcasted_iota(jnp.int32, (BLOCK, BLOCK), 0)
    lane_at = lax.broadcasted_iota(jnp.int32, (BLOCK, BLOCK), 1)
    later, earlier = row_at > lane_at, row_at < lane_at
    upto = (row_at <= lane_at).astype(f32)
    left_lane = lane_at < HEAD_DIM

    def conv(source, low, high, taps, target, at, width):
        ext[pl.ds(8, height), pl.ds(0, width)] = source[:, at].astype(f32)
        ext[pl.ds(0, 8), pl.ds(0, width)] = low[pl.ds(edge - 8, 8), at].astype(f32)
        ext[pl.ds(8 + height, 8), pl.ds(0, width)] = high[pl.ds(0, 8), at].astype(f32)
        weights = taps[:, at]
        for b in range(blocks):
            total = None
            for offset in range(5):
                piece = ext[pl.ds(b * BLOCK + 6 + offset, BLOCK), pl.ds(0, width)]
                if offset != 2:
                    piece = piece * same_ref[pl.ds(b * BLOCK, BLOCK), pl.ds(offset, 1)]
                piece = piece * weights[offset : offset + 1, :]
                total = piece if total is None else total + piece
            total = total / (1.0 + jnp.exp(-total))
            target[pl.ds(b * BLOCK, BLOCK), at] = total.astype(bf16)

    def local_group(g, carry):
        at_wide = pl.ds(pl.multiple_of(g * wide, wide), wide)
        at_state = pl.ds(pl.multiple_of(g * STATE, STATE), STATE)
        conv(value_ref, value_low, value_high, value_taps, values, at_wide, wide)
        conv(entry_ref, entry_low, entry_high, entry_taps, entries, at_state, STATE)
        conv(read_ref, read_low, read_high, read_taps, reads, at_state, STATE)
        whole = None
        ends = None
        for b in range(blocks):
            lanes = pl.ds(b * BLOCK, BLOCK)
            steps, decay = steps_ref[g, :, lanes], decay_ref[g, :, lanes]
            running = jnp.dot(
                decay, upto, precision=exact_prec, preferred_element_type=f32
            )
            totals = jnp.broadcast_to(running[:, BLOCK - 1 :], running.shape)
            ahead = running[:heads]
            behind = running[heads:] - decay[heads:]
            total_f, total_b = totals[:heads], totals[heads:]
            edges = edges_ref[b]
            ids, before, after = edges[0:1], edges[1:2], edges[2:3]
            first, last = edges[3:4], edges[4:5]

            def keep(one, two, value):
                one, two = jnp.broadcast_to(one, value.shape), jnp.broadcast_to(two, value.shape)
                return jnp.where(one == two, value, 0.0)

            pass_f = keep(before, last, jnp.exp(total_f))
            pass_b = keep(after, first, jnp.exp(total_b))
            end_f = keep(ids, last, jnp.exp(total_f - ahead)) * steps[:heads]
            end_b = keep(ids, first, jnp.exp(behind)) * steps[heads:]
            arrive_f = keep(ids, before, jnp.exp(ahead))
            arrive_b = keep(ids, after, jnp.exp(total_b - behind))
            passes = jnp.concatenate([pass_f, pass_b], axis=0)
            passing[g, b] = passes
            whole = passes if whole is None else whole * passes
            vectors[g, b] = jnp.concatenate([ahead, behind, steps], axis=0)
            tall = jnp.concatenate([ahead, behind, arrive_f, arrive_b, end_f, end_b], axis=0)
            tall = jnp.concatenate(
                [tall, jnp.zeros((BLOCK - tall.shape[0], BLOCK), f32)], axis=0
            )
            turned = jnp.transpose(tall)
            columns[g, b] = turned
            value = values[lanes, at_wide].astype(f32)
            entry = entries[lanes, at_state]
            both = []
            for k in range(2):
                weighted = value * spread_heads(turned, (4 + k) * heads, heads, left_lane)
                both.append(
                    lax.dot_general(
                        weighted.astype(bf16),
                        entry,
                        (((0,), (0,)), ((), ())),
                        preferred_element_type=f32,
                    )
                )
                fresh[g, b, k] = both[k]
            ends = both[0] if ends is None else scaled(ends, pass_f, heads) + both[0]
        send_a[g, 0] = ends.astype(bf16)
        starts = fresh[g, blocks - 1, 1]
        for b in range(blocks - 2, -1, -1):
            starts = scaled(starts, passing[g, b][heads:], heads) + fresh[g, b, 1]
        send_a[g, 1] = starts.astype(bf16)
        decay_a[g] = whole
        return carry

    lax.fori_loop(0, groups, local_group, 0)

    out_a = []
    for i in (1, 2, 3):
        target = (q + i) % 4
        out_a.append(
            remote(
                send_a.at[target],
                recv_a.at[i - 1],
                a_sems.at[0, i - 1],
                a_sems.at[1, i - 1],
                plane[i - 1],
            )
        )
        out_a.append(
            remote(
                decay_a.at[target],
                table_a.at[i - 1],
                a_sems.at[2, i - 1],
                a_sems.at[3, i - 1],
                plane[i - 1],
            )
        )
    for copy in out_a:
        copy.start()

    def diagonal(i, carry):
        g, b = i // blocks, i % blocks
        at_wide = pl.ds(pl.multiple_of(g * wide, wide), wide)
        at_state = pl.ds(pl.multiple_of(g * STATE, STATE), STATE)
        at_rows = pl.ds(pl.multiple_of(b * BLOCK, BLOCK), BLOCK)
        score = lax.dot_general(
            reads[at_rows, at_state],
            entries[at_rows, at_state],
            (((1,), (1,)), ((), ())),
            preferred_element_type=f32,
        )
        edges = edges_ref[b]
        score = jnp.where(ids_ref[at_rows, :] == edges[0:1], score, 0.0)
        turned, vector = columns[g, b], vectors[g, b]
        value = values[at_rows, at_wide]
        lane = lax.broadcasted_iota(jnp.int32, value.shape, 1) // HEAD_DIM
        total = None
        for h in range(heads):
            spread = jnp.where(
                later,
                turned[:, h : h + 1] - vector[h : h + 1, :],
                vector[heads + h : heads + h + 1, :] - turned[:, heads + h : heads + h + 1],
            )
            strength = jnp.where(earlier, 0.0, vector[2 * heads + h : 2 * heads + h + 1, :])
            strength = strength + jnp.where(
                later, 0.0, vector[3 * heads + h : 3 * heads + h + 1, :]
            )
            mixing = (score * (jnp.exp(spread) * strength)).astype(bf16)
            masked = jnp.where(lane == h, value, jnp.zeros_like(value))
            part = jnp.dot(mixing, masked, preferred_element_type=f32)
            total = part if total is None else total + part
        within[at_rows, at_wide] = total
        return carry

    lax.fori_loop(0, groups * blocks // 2, diagonal, 0)

    for copy in out_a:
        copy.wait_recv()

    def slot_of(member):
        return (q - member + 4) % 4

    table, gathered = [], []
    for member in range(4):
        i = slot_of(member)
        index = (i + 3) % 4
        is_own = i == 0
        safe = jnp.minimum(index, 2)
        own = (jnp.zeros((8, BLOCK), jnp.int32) + i) == 0
        table.append(jnp.where(own, decay_a[q], table_a[safe]))
        own_tall = (jnp.zeros((wide, BLOCK), jnp.int32) + i) == 0
        gathered.append(
            [
                jnp.where(own_tall, send_a[q, k].astype(f32), recv_a[safe, k].astype(f32))
                for k in range(2)
            ]
        )
    sum_f, through = gathered[0][0], table[0]
    for member in (1, 2, 3):
        sum_f = scaled(sum_f, table[member][:heads], heads) + gathered[member][0]
        through = through * table[member]
    sum_b = gathered[3][1]
    for member in (2, 1, 0):
        sum_b = scaled(sum_b, table[member][heads:], heads) + gathered[member][1]
    send_b[0] = sum_f.astype(bf16)
    send_b[1] = sum_b.astype(bf16)
    decay_b[...] = through
    out_b = []
    for i in range(1, depth):
        to = (z + i) % depth
        lower = (z + i) // depth
        out_b.append(
            remote(
                send_b.at[lower], recv_b.at[i - 1], b_sems.at[0, i - 1], b_sems.at[1, i - 1], tower[i - 1]
            )
        )
        out_b.append(
            remote(
                decay_b, table_b.at[i - 1], b_sems.at[2, i - 1], b_sems.at[3, i - 1], tower[i - 1]
            )
        )
    for copy in out_b:
        copy.start()
    lax.fori_loop(groups * blocks // 2, 3 * groups * blocks // 4, diagonal, 0)
    for copy in out_b:
        copy.wait_recv()

    carry_f = jnp.zeros((wide, BLOCK), f32)
    carry_b = jnp.zeros((wide, BLOCK), f32)
    for other in range(depth):
        index = (z - other + depth) % depth
        safe = (index + depth - 1) % depth
        safe = jnp.minimum(safe, depth - 2)
        below = (jnp.zeros((wide, BLOCK), jnp.int32) + (z - other)) > 0
        carry_f = jnp.where(
            below, scaled(carry_f, table_b[safe][:heads], heads) + recv_b[safe].astype(f32), carry_f
        )
    for other in reversed(range(depth)):
        index = (z - other + depth) % depth
        safe = (index + depth - 1) % depth
        safe = jnp.minimum(safe, depth - 2)
        above = (jnp.zeros((wide, BLOCK), jnp.int32) + (other - z)) > 0
        carry_b = jnp.where(
            above, scaled(carry_b, table_b[safe][heads:], heads) + recv_b[safe].astype(f32), carry_b
        )
    for member in range(4):
        send_c[member, 0] = carry_f.astype(bf16)
        carry_f = scaled(carry_f, table[member][:heads], heads) + gathered[member][0]
    for member in (3, 2, 1, 0):
        send_c[member, 1] = carry_b.astype(bf16)
        carry_b = scaled(carry_b, table[member][heads:], heads) + gathered[member][1]
    out_c = []
    for i in (1, 2, 3):
        out_c.append(
            remote(
                send_c.at[(q + i) % 4],
                recv_c.at[i - 1],
                c_sems.at[0, i - 1],
                c_sems.at[1, i - 1],
                plane[i - 1],
            )
        )
    for copy in out_c:
        copy.start()
    lax.fori_loop(3 * groups * blocks // 4, groups * blocks, diagonal, 0)
    for copy in out_c:
        copy.wait_recv()

    def finish(g, carry):
        at_wide = pl.ds(pl.multiple_of(g * wide, wide), wide)
        at_state = pl.ds(pl.multiple_of(g * STATE, STATE), STATE)
        index = (q - g + 4) % 4
        safe = jnp.minimum((index + 3) % 4, 2)
        own = (jnp.zeros((wide, BLOCK), jnp.int32) + index) == 0
        state = [
            jnp.where(own, send_c[q, k].astype(f32), recv_c[safe, k].astype(f32)) for k in range(2)
        ]
        state_f, state_b = state
        for b in range(blocks):
            entering[b, 0] = state_f.astype(bf16)
            state_f = scaled(state_f, passing[g, b][:heads], heads) + fresh[g, b, 0]
        for b in reversed(range(blocks)):
            entering[b, 1] = state_b.astype(bf16)
            state_b = scaled(state_b, passing[g, b][heads:], heads) + fresh[g, b, 1]

        def block(b, inner):
            at_rows = pl.ds(pl.multiple_of(b * BLOCK, BLOCK), BLOCK)
            read, turned = reads[at_rows, at_state], columns[g, b]
            total = within[at_rows, at_wide]
            for k in range(2):
                carried = lax.dot_general(
                    read, entering[b, k], (((1,), (1,)), ((), ())), preferred_element_type=f32
                )
                total = total + carried * spread_heads(turned, (2 + k) * heads, heads, left_lane)
            gate = gate_ref[at_rows, at_wide].astype(f32)
            total = total * (gate / (1.0 + jnp.exp(-gate)))
            mean = jnp.mean(total * total, axis=1, keepdims=True)
            total = total * lax.rsqrt(mean + norm_eps) * gain_ref[:, at_wide]
            out_ref[at_rows, at_wide] = total.astype(bf16)
            return inner

        lax.fori_loop(0, blocks, block, 0)
        return carry

    lax.fori_loop(0, groups, finish, 0)

    @pl.when(place + 1 < count)
    def _():
        for copy in upward:
            copy.wait_send()

    @pl.when(place > 0)
    def _():
        for copy in downward:
            copy.wait_send()

    swap_down.wait()
    for copy in out_a + out_b + out_c:
        copy.wait_send()


def state_mixer(
    value_rows,
    entry_rows,
    read_rows,
    gate_rows,
    steps,
    decay,
    edges,
    ids,
    same,
    value_taps,
    entry_taps,
    read_taps,
    gain,
    down,
):
    height, value_width = value_rows.shape
    state_width = entry_rows.shape[1]
    groups, pairs, _ = steps.shape
    heads = pairs // 2
    wide = heads * HEAD_DIM
    blocks = height // BLOCK
    depth = lax.axis_size("sp") // 4
    edge = 16
    dma = pltpu.SemaphoreType.DMA
    vmem, anywhere = pl.BlockSpec(memory_space=pltpu.VMEM), pl.BlockSpec(memory_space=pl.ANY)
    return pl.pallas_call(
        states_kernel,
        out_shape=(
            jax.ShapeDtypeStruct((height, value_width), bf16),
            jax.ShapeDtypeStruct((down.shape[0], down.shape[1] // 2), bf16),
        ),
        in_specs=[vmem] * 13 + [anywhere],
        out_specs=(vmem, anywhere),
        scratch_shapes=[
            pltpu.VMEM((height + 16, wide), f32),
            pltpu.VMEM((edge, value_width), bf16),
            pltpu.VMEM((edge, state_width), bf16),
            pltpu.VMEM((edge, state_width), bf16),
            pltpu.VMEM((edge, value_width), bf16),
            pltpu.VMEM((edge, state_width), bf16),
            pltpu.VMEM((edge, state_width), bf16),
            pltpu.VMEM((height, value_width), bf16),
            pltpu.VMEM((height, state_width), bf16),
            pltpu.VMEM((height, state_width), bf16),
            pltpu.VMEM((groups, blocks, 2, wide, STATE), f32),
            pltpu.VMEM((groups, blocks, 4 * heads, BLOCK), f32),
            pltpu.VMEM((groups, blocks, BLOCK, BLOCK), f32),
            pltpu.VMEM((groups, blocks, pairs, BLOCK), f32),
            pltpu.VMEM((height, value_width), f32),
            pltpu.VMEM((blocks, 2, wide, STATE), bf16),
            pltpu.VMEM((groups, 2, wide, STATE), bf16),
            pltpu.VMEM((groups, pairs, BLOCK), f32),
            pltpu.VMEM((3, 2, wide, STATE), bf16),
            pltpu.VMEM((3, pairs, BLOCK), f32),
            pltpu.VMEM((2, wide, STATE), bf16),
            pltpu.VMEM((pairs, BLOCK), f32),
            pltpu.VMEM((depth - 1, wide, STATE), bf16),
            pltpu.VMEM((depth - 1, pairs, BLOCK), f32),
            pltpu.VMEM((4, 2, wide, STATE), bf16),
            pltpu.VMEM((3, 2, wide, STATE), bf16),
            dma((4, 3)),
            dma((4, 3)),
            dma((4, depth - 1)),
            dma((2, 3)),
            dma((2,)),
        ],
        compiler_params=pltpu.CompilerParams(
            collective_id=1, has_side_effects=True, vmem_limit_bytes=48 * 1024 * 1024
        ),
        cost_estimate=pl.CostEstimate(
            flops=60000000000, bytes_accessed=20000000, transcendentals=0
        ),
    )(
        value_rows,
        entry_rows,
        read_rows,
        gate_rows,
        steps,
        decay,
        edges,
        ids,
        same,
        value_taps,
        entry_taps,
        read_taps,
        gain,
        down,
    )


def plain_states(
    head_value_rows,
    entry_map_rows,
    readout_map_rows,
    output_gate_rows,
    step_before_softplus,
    sudden_log_decay,
    document_index,
    head_rate_logarithm,
    head_step_bias,
    value_conv_taps,
    entry_conv_taps,
    readout_conv_taps,
    group_norm_gain,
):
    rows = head_value_rows.shape[0]
    heads = step_before_softplus.shape[1]
    groups = entry_map_rows.shape[1] // STATE
    per_group = heads // groups
    value_width = head_value_rows.shape[1]
    state_width = entry_map_rows.shape[1]
    blocks = rows // BLOCK
    sp_count = lax.axis_size("sp")
    place = lax.axis_index("sp")
    position = place * rows

    taps = value_conv_taps.shape[0]
    half = taps // 2
    ends = jnp.concatenate(
        [
            jnp.concatenate([a[rows - half :], a[:half]], axis=0)
            for a in (head_value_rows, entry_map_rows, readout_map_rows)
        ],
        axis=1,
    )
    low_all = shifted(ends[:half], 1)
    high_all = shifted(ends[half:], -1)
    doc_pad = jnp.pad(document_index, half + 1, constant_values=-1)
    window_ids = lax.dynamic_slice_in_dim(doc_pad, position + 1, rows + 2 * half)
    own_ids = window_ids[half : half + rows]
    prev_id = window_ids[half - 1]
    next_id = window_ids[half + rows]

    def conv(array, weights, start):
        width = array.shape[1]
        extended = jnp.concatenate(
            [low_all[:, start : start + width], array, high_all[:, start : start + width]], axis=0
        )
        weights = weights.astype(f32)
        total = weights[half] * array.astype(f32)
        for offset in range(taps):
            if offset == half:
                continue
            same = (window_ids[offset : offset + rows] == own_ids)[:, None]
            total = total + weights[offset] * jnp.where(
                same, extended[offset : offset + rows].astype(f32), 0.0
            )
        return jax.nn.silu(total).astype(bf16)

    values = conv(head_value_rows, value_conv_taps, 0)
    entries = conv(entry_map_rows, entry_conv_taps, value_width)
    readout = conv(readout_map_rows, readout_conv_taps, value_width + state_width)
    values = values.reshape(blocks, BLOCK, groups, per_group, HEAD_DIM)
    entries = entries.reshape(blocks, BLOCK, groups, STATE)
    readout = readout.reshape(blocks, BLOCK, groups, STATE)

    raw = step_before_softplus.astype(f32).T
    steps = jax.nn.softplus(raw[None] + head_step_bias[:, :, None])
    decay = -jnp.exp(head_rate_logarithm)[:, :, None] * steps + sudden_log_decay.T[None]
    shape = (2, groups, per_group, blocks, BLOCK)
    steps = jnp.transpose(steps.reshape(shape), (0, 3, 1, 2, 4))
    decay = jnp.transpose(decay.reshape(shape), (0, 3, 1, 2, 4))
    at = lax.iota(jnp.int32, BLOCK)
    upto = (at[:, None] <= at[None, :]).astype(f32)
    running = jnp.einsum("kbgrs,st->kbgrt", decay, upto, precision=exact_prec)
    totals = running[..., -1]
    ahead = running[0]
    behind = running[1] - decay[1]

    ids = own_ids.reshape(blocks, BLOCK)
    first_ids, last_ids = ids[:, 0], ids[:, -1]
    before = jnp.concatenate([prev_id[None], last_ids[:-1]])
    after = jnp.concatenate([first_ids[1:], next_id[None]])
    pass_f = jnp.where((before == last_ids)[:, None, None], jnp.exp(totals[0]), 0.0)
    pass_b = jnp.where((after == first_ids)[:, None, None], jnp.exp(totals[1]), 0.0)
    end_f = jnp.where(
        (ids == last_ids[:, None])[:, None, None], jnp.exp(totals[0][..., None] - ahead), 0.0
    ) * steps[0]
    end_b = jnp.where((ids == first_ids[:, None])[:, None, None], jnp.exp(behind), 0.0) * steps[1]
    arrive_f = jnp.where((ids == before[:, None])[:, None, None], jnp.exp(ahead), 0.0)
    arrive_b = jnp.where(
        (ids == after[:, None])[:, None, None], jnp.exp(totals[1][..., None] - behind), 0.0
    )

    own_f, own_b = jnp.prod(pass_f, axis=0), jnp.prod(pass_b, axis=0)

    def fresh_states(weight):
        weighted = values.astype(f32) * jnp.transpose(weight, (0, 3, 1, 2))[..., None]
        return jnp.einsum(
            "bsgrp,bsgn->bgrpn", weighted.astype(bf16), entries, preferred_element_type=f32
        )

    fresh_f = fresh_states(end_f)
    fresh_b = fresh_states(end_b)

    end_state = fresh_f[0]
    for b in range(1, blocks):
        end_state = end_state * pass_f[b][..., None, None] + fresh_f[b]
    start_state = fresh_b[blocks - 1]
    for b in range(blocks - 2, -1, -1):
        start_state = start_state * pass_b[b][..., None, None] + fresh_b[b]
    reach = -(-LONGEST_DOCUMENT // rows)
    in_f = incoming_state(end_state, own_f, 1, reach)
    in_b = incoming_state(start_state, own_b, -1, reach)

    scores = jnp.einsum("btgn,bsgn->bgts", readout, entries, preferred_element_type=f32)
    later = at[:, None] > at[None, :]
    equal = at[:, None] == at[None, :]
    linked = (ids[:, :, None] == ids[:, None, :])[:, None, None]
    spread = jnp.where(
        later,
        ahead[..., :, None] - ahead[..., None, :],
        behind[..., None, :] - behind[..., :, None],
    )
    strength = jnp.where(
        later,
        steps[0][..., None, :],
        jnp.where(equal, steps[0][..., None, :], 0.0) + steps[1][..., None, :],
    )
    weights = jnp.where(linked, jnp.exp(spread) * strength, 0.0)
    mixing = (scores[:, :, None] * weights).astype(bf16)
    output = jnp.einsum("bgrts,bsgrp->bgrtp", mixing, values, preferred_element_type=f32)

    state_f = [in_f]
    for b in range(blocks - 1):
        state_f.append(state_f[-1] * pass_f[b][..., None, None] + fresh_f[b])
    state_b = [in_b]
    for b in range(blocks - 1, 0, -1):
        state_b.append(state_b[-1] * pass_b[b][..., None, None] + fresh_b[b])
    entering_f = jnp.stack([s.astype(bf16) for s in state_f])
    entering_b = jnp.stack([s.astype(bf16) for s in state_b[::-1]])
    carried_f = jnp.einsum("btgn,bgrpn->bgrtp", readout, entering_f, preferred_element_type=f32)
    carried_b = jnp.einsum("btgn,bgrpn->bgrtp", readout, entering_b, preferred_element_type=f32)
    output = output + carried_f * arrive_f[..., None] + carried_b * arrive_b[..., None]

    gated = jnp.transpose(output, (0, 3, 1, 2, 4)).reshape(rows, groups, per_group * HEAD_DIM)
    gated = gated * jax.nn.silu(output_gate_rows.astype(f32)).reshape(gated.shape)
    gated = gated * lax.rsqrt(jnp.mean(gated * gated, axis=2, keepdims=True) + norm_eps)
    normed = (gated.reshape(rows, value_width) * group_norm_gain).astype(bf16)
    return normed


def ring_states(
    head_value_rows,
    entry_map_rows,
    readout_map_rows,
    output_gate_rows,
    step_before_softplus,
    sudden_log_decay,
    document_index,
    head_rate_logarithm,
    head_step_bias,
    value_conv_taps,
    entry_conv_taps,
    readout_conv_taps,
    group_norm_gain,
    down_projection_weight,
):
    rows = head_value_rows.shape[0]
    heads = step_before_softplus.shape[1]
    groups = entry_map_rows.shape[1] // STATE
    blocks = rows // BLOCK
    position = lax.axis_index("sp") * rows
    taps = value_conv_taps.shape[0]
    half = taps // 2
    doc_pad = jnp.pad(document_index, half + 1, constant_values=-1)
    window_ids = lax.dynamic_slice_in_dim(doc_pad, position + 1, rows + 2 * half)
    own_ids = window_ids[half : half + rows]
    same = jnp.stack([window_ids[o : o + rows] == own_ids for o in range(taps)], axis=1)
    same = jnp.pad(same.astype(f32), ((0, 0), (0, 8 - taps)))
    ids = own_ids.reshape(blocks, BLOCK)
    first, last = ids[:, 0], ids[:, -1]
    before = jnp.concatenate([window_ids[half - 1 : half], last[:-1]])
    after = jnp.concatenate([first[1:], window_ids[half + rows : half + rows + 1]])
    flat = [jnp.broadcast_to(v[:, None], ids.shape) for v in (before, after, first, last)]
    edges = jnp.stack([ids] + flat + [ids] * 3, axis=1)
    raw = step_before_softplus.astype(f32).T
    steps = jax.nn.softplus(raw[None] + head_step_bias[:, :, None])
    decay = -jnp.exp(head_rate_logarithm)[:, :, None] * steps + sudden_log_decay.T[None]

    def by_group(array):
        array = array.reshape(2, groups, heads // groups, rows)
        return jnp.transpose(array, (1, 0, 2, 3)).reshape(groups, -1, rows)

    return state_mixer(
        head_value_rows,
        entry_map_rows,
        readout_map_rows,
        output_gate_rows,
        by_group(steps),
        by_group(decay),
        edges,
        own_ids[:, None],
        same,
        value_conv_taps.astype(f32),
        entry_conv_taps.astype(f32),
        readout_conv_taps.astype(f32),
        group_norm_gain[None],
        down_projection_weight,
    )


def per_device(
    head_value_rows,
    entry_map_rows,
    readout_map_rows,
    output_gate_rows,
    step_before_softplus,
    sudden_log_decay,
    document_index,
    head_rate_logarithm,
    head_step_bias,
    value_conv_taps,
    entry_conv_taps,
    readout_conv_taps,
    group_norm_gain,
    mixer_output_weight,
    stream,
    mixer_norm_gain,
    channel_norm_gain,
    up_projection_weight,
    down_projection_weight,
):
    if has_rings():
        up_half = ring_weights(up_projection_weight)
        share = down_projection_weight.shape[1] // 2
        mine = lax.dynamic_slice_in_dim(down_projection_weight, parity() * share, share, 1)
    else:
        up_half = pair_weights(up_projection_weight)
        down_half = pair_weights(down_projection_weight)

    model_width = mixer_output_weight.shape[1]
    rows = head_value_rows.shape[0]
    inputs = (
        head_value_rows,
        entry_map_rows,
        readout_map_rows,
        output_gate_rows,
        step_before_softplus,
        sudden_log_decay,
        document_index,
        head_rate_logarithm,
        head_step_bias,
        value_conv_taps,
        entry_conv_taps,
        readout_conv_taps,
        group_norm_gain,
    )
    if has_rings():
        normed, other = ring_states(*inputs, down_projection_weight)
    else:
        normed = plain_states(*inputs)
    mixer_sum = tp_scatter(jnp.dot(normed, mixer_output_weight, preferred_element_type=f32))
    first_sum = resid_scale * stream.astype(f32) + mixer_sum
    normed_one = norm_rows(first_sum, mixer_norm_gain, model_width)
    if has_rings():
        second_sum = ring_mixer(normed_one, mine, other, up_half)
        return norm_rows(second_sum, channel_norm_gain, model_width)
    piece = rows // PIECES
    returned = [
        pair_swap(
            channel_mixer(
                pair_swap(normed_one[i * piece : (i + 1) * piece]),
                up_half,
                down_half,
            ).astype(bf16)
        )
        for i in range(PIECES)
    ]
    down_sum = channel_mixer(normed_one, up_half, down_half) + jnp.concatenate(returned).astype(f32)
    second_sum = resid_scale * normed_one.astype(f32) + down_sum
    return norm_rows(second_sum, channel_norm_gain, model_width)


def solution(mesh):
    placed = (
        P("sp", "tp"),
        P("sp", "tp"),
        P("sp", "tp"),
        P("sp", "tp"),
        P("sp", "tp"),
        P("sp", "tp"),
        P(),
        P(None, "tp"),
        P(None, "tp"),
        P(None, "tp"),
        P(None, "tp"),
        P(None, "tp"),
        P("tp"),
        P("tp", None),
        P("sp", "tp"),
        P("tp"),
        P("tp"),
        P("sp", "tp"),
        P("sp", "tp"),
    )
    return jax.shard_map(
        per_device, mesh=mesh, in_specs=placed, out_specs=P("sp", "tp"), check_vma=False
    )
```

```python
import jax
import jax.numpy as jnp
from jax import lax
from jax.experimental import pallas as pl
from jax.experimental.pallas import tpu as pltpu
from jax.sharding import PartitionSpec as P

HEAD_DIM = 64
STATE = 128
BLOCK = 128
LONGEST_DOCUMENT = 6144
PIECES = 2


exact_prec = lax.Precision.HIGHEST
norm_eps = 1e-05
resid_scale = 1.4142135623730951
bf16 = jnp.bfloat16
f32 = jnp.float32


def swap(array):
    return lax.ppermute(array, "tp", [(0, 1), (1, 0)])


def tp_scatter(partial):
    if lax.axis_size("tp") != 2:
        return lax.psum_scatter(
            partial.astype(bf16), "tp", scatter_dimension=1, tiled=True
        ).astype(f32)
    me = lax.axis_index("tp")
    width = partial.shape[1] // 2
    rounded = partial.astype(bf16)
    other = lax.dynamic_slice_in_dim(rounded, (1 - me) * width, width, 1)
    mine = lax.dynamic_slice_in_dim(rounded, me * width, width, 1)
    return mine.astype(f32) + swap(other).astype(f32)


def tp_gather(array):
    if lax.axis_size("tp") != 2:
        return lax.all_gather(array, "tp", axis=1, tiled=True)
    other = swap(array)
    first = lax.axis_index("tp") == 0
    return jnp.concatenate(
        [jnp.where(first, array, other), jnp.where(first, other, array)], axis=1
    )


def norm_rows(residual, gain, width):
    sums = jnp.stack([jnp.sum(residual, axis=1), jnp.sum(residual * residual, axis=1)])
    if lax.axis_size("tp") == 2:
        sums = sums + swap(sums)
    else:
        sums = lax.psum(sums, "tp")
    row_mean = sums[0] / width
    row_var = sums[1] / width - row_mean * row_mean
    return ((residual - row_mean[:, None]) * lax.rsqrt(row_var + norm_eps)[:, None] * gain).astype(
        bf16
    )


def pair_swap(array, bit=1):
    count = lax.axis_size("sp")
    return lax.ppermute(array, "sp", [(i, i ^ bit) for i in range(count)])


def pair_weights(weight):
    count = lax.axis_size("sp")
    odd = lax.axis_index("sp") % 2
    width = weight.shape[1] // 2
    mine = lax.dynamic_slice_in_dim(weight, odd * width, width, 1)
    other = pair_swap(lax.dynamic_slice_in_dim(weight, (1 - odd) * width, width, 1))
    both = jnp.concatenate(
        [jnp.where(odd == 0, mine, other), jnp.where(odd == 0, other, mine)], axis=0
    )
    members = [list(range(0, count, 2)), list(range(1, count, 2))]
    return lax.all_gather(both, "sp", axis=0, tiled=True, axis_index_groups=members)


def has_rings():
    return lax.axis_size("tp") == 2 and lax.axis_size("sp") == 2 * RING


MESH_ID = pl.DeviceIdType.MESH
RING = 8


def ring_place(spot, depth):
    far = spot // depth
    return spot + far * (2 * depth - 1 - 2 * spot), far


def ring_flights(remote, size, after, before, store, first, send, recv):
    flights = {}
    for direction, to in enumerate((after, before)):
        for distance in range(size // 2):
            for part in (0, 1):
                if distance == size // 2 - 1 and part != direction:
                    continue
                here = (size - distance) % size if direction == 0 else distance
                there = (here + size - 1) % size if direction == 0 else here + 1
                n = 2 * distance + part
                flights[direction, distance, part] = remote(
                    first[part] if distance == 0 else store.at[2 * here + part],
                    store.at[2 * there + part],
                    send.at[direction, n],
                    recv.at[direction, n],
                    to,
                )
    return flights


def pass_on(flights, distance, turn, flip):
    for direction in (0, 1):
        part = 1 - turn if flip and direction else turn
        if (direction, distance - 1, part) in flights:
            flights[direction, distance - 1, part].wait_recv()
        if (direction, distance, part) in flights:
            flights[direction, distance, part].start()


def twin_norm(remote, twin, sums, gain_ref, store, send_s, recv_s, sems):
    height, width = sums.shape
    cut = 128
    lane = lax.broadcasted_iota(jnp.int32, (cut, 128), 1)
    for i in range(height // cut):
        value = sums[pl.ds(i * cut, cut), :]
        total = jnp.sum(value, axis=1, keepdims=True)
        power = jnp.sum(value * value, axis=1, keepdims=True)
        send_s[pl.ds(i * cut, cut), :] = jnp.where(lane == 0, total, power)
    stats_out = remote(send_s, recv_s, sems.at[0], sems.at[1], twin)
    stats_out.start()
    stats_out.wait_recv()
    for i in range(height // cut):
        at = pl.ds(i * cut, cut)
        stats = (send_s[at, :] + recv_s[at, :]) / (2 * width)
        mean = stats[:, 0:1]
        scale = lax.rsqrt(stats[:, 1:2] - mean * mean + norm_eps)
        store(at, ((sums[at, :] - mean) * scale * gain_ref[...]).astype(bf16))
    stats_out.wait_send()


def mixer_kernel(
    rows_ref,
    gain_ref,
    down_ref,
    other_ref,
    up_ref,
    up_all_ref,
    out_ref,
    sum_ref,
    send_s,
    recv_s,
    down,
    up,
    rows,
    squared,
    local,
    send_t,
    recv_t,
    keep_o,
    keep_x,
    send_x,
    recv_x,
    up_sem,
    own_sem,
    row_send,
    row_recv,
    ring_send,
    ring_recv,
    t_sems,
    x_sems,
    first_sems,
):
    count = lax.axis_size("sp")
    depth = count // 4
    size = count // 2
    place = lax.axis_index("sp")
    me = lax.axis_index("tp")
    z, y, x = place // 4, (place // 2) % 2, place % 2
    spot = z + y * (2 * depth - 1 - 2 * z)
    height, width = rows_ref.shape
    half = height // 2
    hidden_width = up.shape[1]
    piece = down.shape[1]
    tile = 2 * piece
    mine = pl.ds(pl.multiple_of(x * hidden_width, hidden_width), hidden_width)

    def member(where):
        level, far = ring_place(where, depth)
        return level * 4 + far * 2 + x

    after = (member((spot + 1) % size), me)
    before = (member((spot + size - 1) % size), me)
    across = place + 1 - 2 * x
    twin = (place, 1 - me)
    opposite = (across, me)

    barrier = pltpu.get_barrier_semaphore()
    near = (after, before, twin, opposite)
    for device in near:
        pl.semaphore_signal(barrier, inc=1, device_id=device, device_id_type=MESH_ID)
    pl.semaphore_wait(barrier, len(near))

    def remote(source, target, send, recv, device):
        return pltpu.make_async_remote_copy(
            src_ref=source,
            dst_ref=target,
            send_sem=send,
            recv_sem=recv,
            device_id=device,
            device_id_type=MESH_ID,
        )

    pending = []

    first = (down_ref.at[:, mine], other_ref)
    flights = ring_flights(remote, size, after, before, down, first, ring_send, ring_recv)
    pending.extend(flights.values())
    for direction in (0, 1):
        for part in (0, 1) if direction == 0 else (1, 0):
            flights[direction, 0, part].start()

    def forward(distance, turn):
        pass_on(flights, distance, turn, True)

    loads = []
    for i in range(size):
        base = member((spot + i) % size)
        for part, source in enumerate((base, base + 1 - 2 * x)):
            loads.append(
                pltpu.make_async_copy(
                    up_ref.at[:, mine] if i + part == 0 else up_all_ref.at[2 * i + part],
                    up.at[pl.ds(pl.multiple_of(source * piece, piece), piece)],
                    up_sem.at[2 * i + part],
                )
            )
    own = [
        pltpu.make_async_copy(down_ref.at[:, mine], down.at[0], own_sem.at[0]),
        pltpu.make_async_copy(other_ref, down.at[1], own_sem.at[1]),
    ]
    my_columns = pl.ds(pl.multiple_of(me * width, width), width)
    parts = [pl.ds(i * half, half) for i in range(4)]
    to_twin = remote(
        rows_ref, rows.at[pl.ds(0, height), my_columns], row_send.at[0], row_recv.at[0], twin
    )
    outward = [
        remote(
            rows_ref.at[parts[i]],
            rows.at[parts[2 + i], my_columns],
            row_send.at[1 + i],
            row_recv.at[1 + i],
            opposite,
        )
        for i in range(2)
    ]
    inward = [
        remote(
            rows.at[parts[2 + i], my_columns],
            rows.at[parts[2 + i], my_columns],
            row_send.at[3 + i],
            row_recv.at[3 + i],
            twin,
        )
        for i in range(2)
    ]
    for copy in [to_twin] + outward:
        copy.start()
    pending.extend([to_twin] + outward + inward)
    for copy in loads + own:
        copy.start()
    rows[pl.ds(0, height), my_columns] = rows_ref[...]

    to_twin.wait_recv()
    for copy in loads:
        copy.wait()

    def raise_rows(start, length):
        def body(i, carry):
            columns = pl.ds(pl.multiple_of(i * tile, tile), tile)
            value = jnp.dot(
                rows[pl.ds(start, length), :], up[:, columns], preferred_element_type=f32
            )
            value = jnp.maximum(value, 0.0)
            squared[pl.ds(start, length), columns] = (value * value).astype(bf16)
            return carry

        lax.fori_loop(0, hidden_width // tile, body, 0)

    raise_rows(0, height)
    forward(1, 0)
    outward[0].wait_recv()
    inward[0].start()
    forward(1, 1)
    inward[0].wait_recv()
    raise_rows(height, half)
    forward(2, 0)
    outward[1].wait_recv()
    inward[1].start()
    inward[1].wait_recv()
    raise_rows(height + half, half)
    for copy in own:
        copy.wait()

    def owner(where):
        level, _ = ring_place(where, depth)
        return level // (depth // 2)

    def product(slot, start):
        return lax.dot_general(
            squared[pl.ds(start, height), :],
            down[pl.ds(2 * slot, 2)].reshape(tile, hidden_width),
            (((1,), (1,)), ((), ())),
            preferred_element_type=f32,
        )

    spare = size // 2
    handed = [
        remote(
            send_t.at[2 * (i % spare) + part],
            recv_t.at[2 * (i % spare) + part],
            t_sems.at[0, 2 * (i % spare) + part],
            t_sems.at[1, 2 * (i % spare) + part],
            twin,
        )
        for i in range(size)
        for part in (0, 1)
    ]
    returned = [
        remote(
            send_x.at[i % spare],
            recv_x.at[i % spare],
            x_sems.at[0, i % spare],
            x_sems.at[1, i % spare],
            opposite,
        )
        for i in range(size)
    ]
    is_ours = [owner((spot + i) % size) == me for i in range(size)]
    is_theirs = [owner((spot + i) % size) != me for i in range(size)]

    def lower(i):
        k = i % spare
        keep_x[...] = product(i, height)

        @pl.when(is_theirs[i])
        def _():
            send_t[2 * k] = keep_x[...].astype(bf16)
            handed[2 * i].start()

        keep_o[...] = product(i, 0).astype(bf16)

        @pl.when(is_ours[i])
        def _():
            local[k] = keep_o[...]
            handed[2 * i].wait_recv()
            send_x[k] = (keep_x[...] + recv_t[2 * k].astype(f32)).astype(bf16)
            returned[i].start()

        @pl.when(is_theirs[i])
        def _():
            send_t[2 * k + 1] = keep_o[...]
            handed[2 * i + 1].start()

    sum_ref[...] = resid_scale * rows_ref[...].astype(f32)

    def settle(i):
        k = i % spare

        @pl.when(is_ours[i])
        def _():
            base = member((spot + i) % size) - me * (count // 2)
            pair = base + 1 - 2 * x
            handed[2 * i + 1].wait_recv()
            returned[i].wait_recv()
            for part, spot_at in enumerate((base, pair)):
                columns = pl.ds(part * piece, piece)
                swapped = pl.ds((1 - part) * piece, piece)
                target = pl.ds(pl.multiple_of(spot_at * piece, piece), piece)
                sum_ref[:, target] += (
                    local[k, :, columns].astype(f32)
                    + recv_t[2 * k + 1, :, columns].astype(f32)
                    + recv_x[k, :, swapped].astype(f32)
                )

    lower(0)
    lower(1)
    lower(size - 1)
    forward(2, 1)
    lower(2)
    lower(size - 2)
    forward(3, 0)
    settle(0)
    settle(1)
    settle(size - 1)
    forward(3, 1)
    lower(3)
    lower(size - 3)
    settle(2)
    settle(size - 2)
    forward(4, 0)
    lower(4)
    settle(3)
    settle(size - 3)
    settle(4)

    def store_out(at, value):
        out_ref[at, :] = value

    twin_norm(remote, twin, sum_ref, gain_ref, store_out, send_s, recv_s, first_sems)
    for copy in pending:
        copy.wait_send()
    for i in range(size):

        @pl.when(is_theirs[i])
        def _(i=i):
            handed[2 * i].wait_send()
            handed[2 * i + 1].wait_send()

        @pl.when(is_ours[i])
        def _(i=i):
            returned[i].wait_send()


def ring_mixer(rows, gain, down, other, up, up_all):
    count = lax.axis_size("sp")
    height, width = rows.shape
    size = count // 2
    piece, hidden = other.shape
    tile, spare = 2 * piece, size // 2
    dma = pltpu.SemaphoreType.DMA
    vmem, anywhere = pl.BlockSpec(memory_space=pltpu.VMEM), pl.BlockSpec(memory_space=pl.ANY)
    return pl.pallas_call(
        mixer_kernel,
        out_shape=jax.ShapeDtypeStruct((height, width), bf16),
        in_specs=[vmem, vmem] + [anywhere] * 4,
        out_specs=vmem,
        scratch_shapes=[
            pltpu.VMEM((height, width), f32),
            pltpu.VMEM((height, 128), f32),
            pltpu.VMEM((height, 128), f32),
            pltpu.VMEM((count, piece, hidden), bf16),
            pltpu.VMEM((2 * width, hidden), bf16),
            pltpu.VMEM((2 * height, 2 * width), bf16),
            pltpu.VMEM((2 * height, hidden), bf16),
            pltpu.VMEM((spare, height, tile), bf16),
            pltpu.VMEM((2 * spare, height, tile), bf16),
            pltpu.VMEM((2 * spare, height, tile), bf16),
            pltpu.VMEM((height, tile), bf16),
            pltpu.VMEM((height, tile), f32),
            pltpu.VMEM((spare, height, tile), bf16),
            pltpu.VMEM((spare, height, tile), bf16),
            dma((count,)),
            dma((2,)),
            dma((5,)),
            dma((5,)),
            dma((2, size)),
            dma((2, size)),
            dma((2, 2 * spare)),
            dma((2, spare)),
            dma((2,)),
        ],
        compiler_params=pltpu.CompilerParams(
            collective_id=0, has_side_effects=True, vmem_limit_bytes=62 * 1024 * 1024
        ),
        cost_estimate=pl.CostEstimate(
            flops=8 * height * 2 * width * hidden, bytes_accessed=30000000, transcendentals=0
        ),
    )(rows, gain, down, other, up, up_all)


def channel_mixer(rows, up, down):
    hidden = jnp.dot(tp_gather(rows), up, preferred_element_type=f32)
    squared = jnp.square(jax.nn.relu(hidden)).astype(bf16)
    part = lax.dot_general(squared, down, (((1,), (1,)), ((), ())), preferred_element_type=f32)
    return tp_scatter(part)


def shifted(array, step):
    count = lax.axis_size("sp")
    if step > 0:
        pairs = [(i, i + step) for i in range(count - step)]
    else:
        pairs = [(i, i + step) for i in range(-step, count)]
    return lax.ppermute(array, "sp", pairs)


def with_decay(state, through):
    heads = through.size
    flat = state.reshape(heads, -1).astype(bf16)
    through = through.reshape(heads, 1)
    high = through.astype(bf16)
    middle = (through - high.astype(f32)).astype(bf16)
    low = (through - high.astype(f32) - middle.astype(f32)).astype(bf16)
    terms = jnp.concatenate([high, middle, low], axis=1)
    return jnp.concatenate([flat, jnp.pad(terms, ((0, 0), (0, 125)))], axis=1)


def apart(packed, shape):
    terms = packed[:, -128:].astype(f32)
    through = terms[:, 0] + (terms[:, 1] + terms[:, 2])
    return packed[:, :-128].astype(f32).reshape(shape), through.reshape(shape[:2])


def incoming_state(end_state, own_pass, direction, reach):
    count = lax.axis_size("sp")
    shape = end_state.shape
    state, through = apart(shifted(with_decay(end_state, own_pass), direction), shape)
    covered = 1
    while covered < min(reach, count - 1):
        more, further = apart(shifted(with_decay(state, through), direction * covered), shape)
        state = state + through[..., None, None] * more
        through = through * further
        covered *= 2
    return state


def scaled(state, scale, heads):
    head_dim = state.shape[0] // heads
    return jnp.concatenate(
        [
            state[h * head_dim : (h + 1) * head_dim] * scale[h : h + 1, :]
            for h in range(heads)
        ],
        axis=0,
    )


def spread_heads(columns, first, heads, lane):
    parts = []
    for h in range(0, heads, 2):
        parts.append(
            jnp.where(
                lane, columns[:, first + h : first + h + 1], columns[:, first + h + 1 : first + h + 2]
            )
        )
    return jnp.concatenate(parts, axis=1)


def states_kernel(
    value_ref,
    entry_ref,
    read_ref,
    gate_ref,
    steps_ref,
    decay_ref,
    index_ref,
    value_taps,
    entry_taps,
    read_taps,
    gain_ref,
    down_ref,
    up_ref,
    stream_ref,
    out_weight_ref,
    mixer_gain_ref,
    out_ref,
    other_ref,
    up_all,
    value_in,
    entry_in,
    read_in,
    gate_in,
    stream_in,
    out_weight,
    normed,
    recv_o,
    send_s,
    recv_s,
    edges_ref,
    same_ref,
    ext,
    value_low,
    entry_low,
    read_low,
    value_high,
    entry_high,
    read_high,
    values,
    entries,
    reads,
    fresh,
    vectors,
    columns,
    passing,
    within,
    entering,
    send_a,
    decay_a,
    recv_a,
    table_a,
    send_b,
    decay_b,
    recv_b,
    table_b,
    send_c,
    recv_c,
    halo_sems,
    a_sems,
    b_sems,
    c_sems,
    swap_sems,
    ring_send,
    ring_recv,
    load_sems,
    first_sems,
):
    count = lax.axis_size("sp")
    place = lax.axis_index("sp")
    me = lax.axis_index("tp")
    depth = count // 4
    z, q = place // 4, place % 4
    height = value_ref.shape[0]
    groups = steps_ref.shape[0]
    blocks = height // BLOCK
    heads = steps_ref.shape[1] // 2
    wide = heads * HEAD_DIM
    edge = value_low.shape[0]

    plane = [(z * 4 + (q + i) % 4, me) for i in (1, 2, 3)]
    tower = [(((z + i) % depth) * 4 + q, me) for i in range(1, depth)]
    up_place, down_place = (place + 1, me), (place - 1, me)
    twin = (place, 1 - me)
    loads = [
        pltpu.make_async_copy(source, target, load_sems.at[i])
        for i, (source, target) in enumerate(
            (
                (value_ref, value_in),
                (entry_ref, entry_in),
                (read_ref, read_in),
                (gate_ref, gate_in),
                (stream_ref, stream_in),
                (out_weight_ref, out_weight),
            )
        )
    ]
    for copy in loads:
        copy.start()

    barrier = pltpu.get_barrier_semaphore()

    @pl.when(place + 1 < count)
    def _():
        pl.semaphore_signal(barrier, inc=1, device_id=up_place, device_id_type=MESH_ID)

    @pl.when(place > 0)
    def _():
        pl.semaphore_signal(barrier, inc=1, device_id=down_place, device_id_type=MESH_ID)

    for device in plane + tower + [twin]:
        pl.semaphore_signal(barrier, inc=1, device_id=device, device_id_type=MESH_ID)

    @pl.when((place > 0) & (place + 1 < count))
    def _():
        pl.semaphore_wait(barrier, len(plane) + len(tower) + 3)

    @pl.when((place == 0) | (place + 1 == count))
    def _():
        pl.semaphore_wait(barrier, len(plane) + len(tower) + 2)

    def remote(source, target, send, recv, device):
        return pltpu.make_async_remote_copy(
            src_ref=source,
            dst_ref=target,
            send_sem=send,
            recv_sem=recv,
            device_id=device,
            device_id_type=MESH_ID,
        )

    raw = (value_ref, entry_ref, read_ref)
    lows, highs = (value_low, entry_low, read_low), (value_high, entry_high, read_high)
    upward = [
        remote(
            raw[i].at[pl.ds(height - edge, edge)],
            lows[i],
            halo_sems.at[0, i],
            halo_sems.at[1, i],
            up_place,
        )
        for i in range(3)
    ]
    downward = [
        remote(
            raw[i].at[pl.ds(0, edge)], highs[i], halo_sems.at[2, i], halo_sems.at[3, i], down_place
        )
        for i in range(3)
    ]

    @pl.when(place + 1 < count)
    def _():
        for copy in upward:
            copy.start()

    @pl.when(place > 0)
    def _():
        for copy in downward:
            copy.start()

    x = place % 2
    share = other_ref.shape[1]
    mine = pl.ds(pl.multiple_of(x * share, share), share)
    theirs = pl.ds(pl.multiple_of((1 - x) * share, share), share)
    opposite = (place + 1 - 2 * x, me)
    swap_up = remote(
        up_ref.at[:, theirs], up_all.at[1], swap_sems.at[2], swap_sems.at[3], opposite
    )
    swap_down = remote(
        down_ref.at[:, theirs], other_ref, swap_sems.at[0], swap_sems.at[1], opposite
    )
    size = count // 2
    y = (place // 2) % 2
    spot = z + y * (2 * depth - 1 - 2 * z)

    def member(where):
        level, far = ring_place(where, depth)
        return level * 4 + far * 2 + x

    flights = ring_flights(
        remote,
        size,
        (member((spot + 1) % size), me),
        (member((spot + size - 1) % size), me),
        up_all,
        (up_ref.at[:, mine], up_all.at[1]),
        ring_send,
        ring_recv,
    )
    swap_up.start()
    for direction in (0, 1):
        flights[direction, 0, 0].start()
    swap_down.start()

    def forward(distance, turn):
        pass_on(flights, distance, turn, False)

    @pl.when(place == 0)
    def _():
        for low in lows:
            low[...] = jnp.zeros_like(low)

    @pl.when(place + 1 == count)
    def _():
        for high in highs:
            high[...] = jnp.zeros_like(high)

    @pl.when(place > 0)
    def _():
        for copy in upward:
            copy.wait_recv()

    @pl.when(place + 1 < count)
    def _():
        for copy in downward:
            copy.wait_recv()

    row_at = lax.broadcasted_iota(jnp.int32, (BLOCK, BLOCK), 0)
    lane_at = lax.broadcasted_iota(jnp.int32, (BLOCK, BLOCK), 1)
    later, earlier = row_at > lane_at, row_at < lane_at
    upto = (row_at <= lane_at).astype(f32)
    left_lane = lane_at < HEAD_DIM

    def conv(source, low, high, taps, target, at, width):
        ext[pl.ds(8, height), pl.ds(0, width)] = source[:, at].astype(f32)
        ext[pl.ds(0, 8), pl.ds(0, width)] = low[pl.ds(edge - 8, 8), at].astype(f32)
        ext[pl.ds(8 + height, 8), pl.ds(0, width)] = high[pl.ds(0, 8), at].astype(f32)
        weights = taps[:, at].astype(f32)
        for b in range(blocks):
            total = None
            for offset in range(5):
                piece = ext[pl.ds(b * BLOCK + 6 + offset, BLOCK), pl.ds(0, width)]
                if offset != 2:
                    piece = piece * same_ref[pl.ds(b * BLOCK, BLOCK), pl.ds(offset, 1)]
                piece = piece * weights[offset : offset + 1, :]
                total = piece if total is None else total + piece
            total = total / (1.0 + jnp.exp(-total))
            target[pl.ds(b * BLOCK, BLOCK), at] = total.astype(bf16)

    out_a = []
    for i in (1, 2, 3):
        target = (q + i) % 4
        out_a.append(
            remote(
                send_a.at[target],
                recv_a.at[i - 1],
                a_sems.at[0, i - 1],
                a_sems.at[1, i - 1],
                plane[i - 1],
            )
        )
        out_a.append(
            remote(
                decay_a.at[target],
                table_a.at[i - 1],
                a_sems.at[2, i - 1],
                a_sems.at[3, i - 1],
                plane[i - 1],
            )
        )

    def local_group(i, carry):
        g = (q + 1 + i) % groups
        at_wide = pl.ds(pl.multiple_of(g * wide, wide), wide)
        at_state = pl.ds(pl.multiple_of(g * STATE, STATE), STATE)
        conv(value_in, value_low, value_high, value_taps, values, at_wide, wide)
        conv(entry_in, entry_low, entry_high, entry_taps, entries, at_state, STATE)
        conv(read_in, read_low, read_high, read_taps, reads, at_state, STATE)
        whole = None
        ends = None
        for b in range(blocks):
            lanes = pl.ds(b * BLOCK, BLOCK)
            steps, decay = steps_ref[g, :, lanes], decay_ref[g, :, lanes]
            running = jnp.dot(
                decay, upto, precision=exact_prec, preferred_element_type=f32
            )
            totals = jnp.broadcast_to(running[:, BLOCK - 1 :], running.shape)
            ahead = running[:heads]
            behind = running[heads:] - decay[heads:]
            total_f, total_b = totals[:heads], totals[heads:]
            edges = edges_ref[b]
            ids, before, after = edges[0:1], edges[1:2], edges[2:3]
            first, last = edges[3:4], edges[4:5]

            def keep(one, two, value):
                one, two = jnp.broadcast_to(one, value.shape), jnp.broadcast_to(two, value.shape)
                return jnp.where(one == two, value, 0.0)

            pass_f = keep(before, last, jnp.exp(total_f))
            pass_b = keep(after, first, jnp.exp(total_b))
            end_f = keep(ids, last, jnp.exp(total_f - ahead)) * steps[:heads]
            end_b = keep(ids, first, jnp.exp(behind)) * steps[heads:]
            arrive_f = keep(ids, before, jnp.exp(ahead))
            arrive_b = keep(ids, after, jnp.exp(total_b - behind))
            passes = jnp.concatenate([pass_f, pass_b], axis=0)
            passing[g, b] = passes
            whole = passes if whole is None else whole * passes
            vectors[g, b] = jnp.concatenate([ahead, behind, steps], axis=0)
            tall = jnp.concatenate([ahead, behind, arrive_f, arrive_b, end_f, end_b], axis=0)
            tall = jnp.concatenate(
                [tall, jnp.zeros((BLOCK - tall.shape[0], BLOCK), f32)], axis=0
            )
            turned = jnp.transpose(tall)
            columns[g, b] = turned
            value = values[lanes, at_wide].astype(f32)
            entry = entries[lanes, at_state]
            both = []
            for k in range(2):
                weighted = value * spread_heads(turned, (4 + k) * heads, heads, left_lane)
                both.append(
                    lax.dot_general(
                        weighted.astype(bf16),
                        entry,
                        (((0,), (0,)), ((), ())),
                        preferred_element_type=f32,
                    )
                )
                fresh[g, b, k] = both[k]
            ends = both[0] if ends is None else scaled(ends, pass_f, heads) + both[0]
        send_a[g, 0] = ends.astype(bf16)
        starts = fresh[g, blocks - 1, 1]
        for b in range(blocks - 2, -1, -1):
            starts = scaled(starts, passing[g, b][heads:], heads) + fresh[g, b, 1]
        send_a[g, 1] = starts.astype(bf16)
        decay_a[g] = whole

        for k in range(groups - 1):

            @pl.when(i == k)
            def _(k=k):
                out_a[2 * k].start()
                out_a[2 * k + 1].start()

        @pl.when(i == 0)
        def _():
            swap_up.wait_recv()
            for direction in (0, 1):
                flights[direction, 0, 1].start()
            forward(1, 0)

        @pl.when(i == 2)
        def _():
            forward(1, 1)

        return carry

    def index_row(b):
        at = jnp.clip(place * blocks + b, 0, count * blocks - 1)
        row = index_ref[pl.ds(at, 1), :].astype(f32)
        outside = (place * blocks + b < 0) | (place * blocks + b >= count * blocks)
        return jnp.where(outside, jnp.full_like(row, -1.0), row)

    index_rows = [index_row(b) for b in range(-1, blocks + 1)]
    for b in range(blocks):
        prior, row, following = index_rows[b : b + 3]
        line = row.shape
        first = jnp.broadcast_to(row[:, :1], line)
        last = jnp.broadcast_to(row[:, BLOCK - 1 :], line)
        before = jnp.broadcast_to(prior[:, BLOCK - 1 :], line)
        after = jnp.broadcast_to(following[:, :1], line)
        edges_ref[b] = jnp.concatenate([row, before, after, first, last] + [row] * 3, axis=0)
        long = jnp.concatenate([prior, row, following], axis=1)
        moved = [long[:, BLOCK + o - 2 : 2 * BLOCK + o - 2] for o in range(5)]
        flags = [jnp.where(m == row, 1.0, 0.0) for m in moved] + [row]
        zeros = jnp.zeros((BLOCK - len(flags), BLOCK), f32)
        same_ref[pl.ds(b * BLOCK, BLOCK), :] = jnp.transpose(
            jnp.concatenate(flags + [zeros], axis=0)
        )
    for copy in loads[:3]:
        copy.wait()
    lax.fori_loop(0, groups, local_group, 0)

    def diagonal(i, carry):
        g, b = i // blocks, i % blocks
        at_wide = pl.ds(pl.multiple_of(g * wide, wide), wide)
        at_state = pl.ds(pl.multiple_of(g * STATE, STATE), STATE)
        at_rows = pl.ds(pl.multiple_of(b * BLOCK, BLOCK), BLOCK)
        score = lax.dot_general(
            reads[at_rows, at_state],
            entries[at_rows, at_state],
            (((1,), (1,)), ((), ())),
            preferred_element_type=f32,
        )
        edges = edges_ref[b]
        score = jnp.where(same_ref[at_rows, 5:6] == edges[0:1], score, 0.0)
        turned, vector = columns[g, b], vectors[g, b]
        value = values[at_rows, at_wide]
        lane = lax.broadcasted_iota(jnp.int32, value.shape, 1) // HEAD_DIM
        total = None
        for h in range(heads):
            spread = jnp.where(
                later,
                turned[:, h : h + 1] - vector[h : h + 1, :],
                vector[heads + h : heads + h + 1, :] - turned[:, heads + h : heads + h + 1],
            )
            strength = jnp.where(earlier, 0.0, vector[2 * heads + h : 2 * heads + h + 1, :])
            strength = strength + jnp.where(
                later, 0.0, vector[3 * heads + h : 3 * heads + h + 1, :]
            )
            mixing = (score * (jnp.exp(spread) * strength)).astype(bf16)
            masked = jnp.where(lane == h, value, jnp.zeros_like(value))
            part = jnp.dot(mixing, masked, preferred_element_type=f32)
            total = part if total is None else total + part
        within[at_rows, at_wide] = total
        return carry

    for copy in out_a:
        copy.wait_recv()

    def slot_of(member):
        return (q - member + 4) % 4

    table, gathered = [], []
    for member in range(4):
        i = slot_of(member)
        index = (i + 3) % 4
        is_own = i == 0
        safe = jnp.minimum(index, 2)
        own = (jnp.zeros((8, BLOCK), jnp.int32) + i) == 0
        table.append(jnp.where(own, decay_a[q], table_a[safe]))
        own_tall = (jnp.zeros((wide, BLOCK), jnp.int32) + i) == 0
        gathered.append(
            [
                jnp.where(own_tall, send_a[q, k].astype(f32), recv_a[safe, k].astype(f32))
                for k in range(2)
            ]
        )
    sum_f, through = gathered[0][0], table[0]
    for member in (1, 2, 3):
        sum_f = scaled(sum_f, table[member][:heads], heads) + gathered[member][0]
        through = through * table[member]
    sum_b = gathered[3][1]
    for member in (2, 1, 0):
        sum_b = scaled(sum_b, table[member][heads:], heads) + gathered[member][1]
    send_b[0] = sum_f.astype(bf16)
    send_b[1] = sum_b.astype(bf16)
    decay_b[...] = through
    out_b = []
    for i in range(1, depth):
        to = (z + i) % depth
        lower = (z + i) // depth
        out_b.append(
            remote(
                send_b.at[lower], recv_b.at[i - 1], b_sems.at[0, i - 1], b_sems.at[1, i - 1], tower[i - 1]
            )
        )
        out_b.append(
            remote(
                decay_b, table_b.at[i - 1], b_sems.at[2, i - 1], b_sems.at[3, i - 1], tower[i - 1]
            )
        )
    for copy in out_b:
        copy.start()
    lax.fori_loop(0, groups * blocks // 2, diagonal, 0)
    forward(2, 0)
    for copy in out_b:
        copy.wait_recv()

    carry_f = jnp.zeros((wide, BLOCK), f32)
    carry_b = jnp.zeros((wide, BLOCK), f32)
    for other in range(depth):
        index = (z - other + depth) % depth
        safe = (index + depth - 1) % depth
        safe = jnp.minimum(safe, depth - 2)
        below = (jnp.zeros((wide, BLOCK), jnp.int32) + (z - other)) > 0
        carry_f = jnp.where(
            below, scaled(carry_f, table_b[safe][:heads], heads) + recv_b[safe].astype(f32), carry_f
        )
    for other in reversed(range(depth)):
        index = (z - other + depth) % depth
        safe = (index + depth - 1) % depth
        safe = jnp.minimum(safe, depth - 2)
        above = (jnp.zeros((wide, BLOCK), jnp.int32) + (other - z)) > 0
        carry_b = jnp.where(
            above, scaled(carry_b, table_b[safe][heads:], heads) + recv_b[safe].astype(f32), carry_b
        )
    for member in range(4):
        send_c[member, 0] = carry_f.astype(bf16)
        carry_f = scaled(carry_f, table[member][:heads], heads) + gathered[member][0]
    for member in (3, 2, 1, 0):
        send_c[member, 1] = carry_b.astype(bf16)
        carry_b = scaled(carry_b, table[member][heads:], heads) + gathered[member][1]
    out_c = []
    for i in (1, 2, 3):
        out_c.append(
            remote(
                send_c.at[(q + i) % 4],
                recv_c.at[i - 1],
                c_sems.at[0, i - 1],
                c_sems.at[1, i - 1],
                plane[i - 1],
            )
        )
    for copy in out_c:
        copy.start()
    lax.fori_loop(groups * blocks // 2, groups * blocks, diagonal, 0)
    forward(2, 1)
    for copy in out_c:
        copy.wait_recv()

    def finish(g, carry):
        at_wide = pl.ds(pl.multiple_of(g * wide, wide), wide)
        at_state = pl.ds(pl.multiple_of(g * STATE, STATE), STATE)
        index = (q - g + 4) % 4
        safe = jnp.minimum((index + 3) % 4, 2)
        own = (jnp.zeros((wide, BLOCK), jnp.int32) + index) == 0
        state = [
            jnp.where(own, send_c[q, k].astype(f32), recv_c[safe, k].astype(f32)) for k in range(2)
        ]
        state_f, state_b = state
        for b in range(blocks):
            entering[b, 0] = state_f.astype(bf16)
            state_f = scaled(state_f, passing[g, b][:heads], heads) + fresh[g, b, 0]
        for b in reversed(range(blocks)):
            entering[b, 1] = state_b.astype(bf16)
            state_b = scaled(state_b, passing[g, b][heads:], heads) + fresh[g, b, 1]

        def block(b, inner):
            at_rows = pl.ds(pl.multiple_of(b * BLOCK, BLOCK), BLOCK)
            read, turned = reads[at_rows, at_state], columns[g, b]
            total = within[at_rows, at_wide]
            for k in range(2):
                carried = lax.dot_general(
                    read, entering[b, k], (((1,), (1,)), ((), ())), preferred_element_type=f32
                )
                total = total + carried * spread_heads(turned, (2 + k) * heads, heads, left_lane)
            gate = gate_in[at_rows, at_wide].astype(f32)
            total = total * (gate / (1.0 + jnp.exp(-gate)))
            mean = jnp.mean(total * total, axis=1, keepdims=True)
            total = total * lax.rsqrt(mean + norm_eps) * gain_ref[:, at_wide]
            normed[at_rows, at_wide] = total.astype(bf16)
            return inner

        lax.fori_loop(0, blocks, block, 0)

        @pl.when(g == 1)
        def _():
            forward(3, 0)

        return carry

    for copy in loads[3:]:
        copy.wait()
    lax.fori_loop(0, groups, finish, 0)

    width = out_ref.shape[1]
    strip = width // 2

    def project(owner_of, store):
        def body(i, carry):
            columns = pl.ds(pl.multiple_of(i * strip, strip), strip)
            taken = pl.ds(pl.multiple_of(owner_of * width + i * strip, strip), strip)
            value = jnp.dot(normed[...], out_weight[:, taken], preferred_element_type=f32)
            store(columns, value.astype(bf16))
            return carry

        lax.fori_loop(0, width // strip, body, 0)

    sums_out = remote(values, recv_o, first_sems.at[0], first_sems.at[1], twin)

    def store_sent(columns, value):
        values[:, columns] = value

    def store_own(columns, value):
        within[:, columns] = resid_scale * stream_in[:, columns].astype(f32) + value.astype(f32)

    project(1 - me, store_sent)
    sums_out.start()
    project(me, store_own)
    forward(3, 1)
    sums_out.wait_recv()
    for b in range(blocks):
        at = pl.ds(b * BLOCK, BLOCK)
        within[at, :] += recv_o[at, :].astype(f32)

    def store_out(at, value):
        out_ref[at, :] = value

    stats = first_sems.at[pl.ds(2, 2)]
    twin_norm(remote, twin, within, mixer_gain_ref, store_out, send_s, recv_s, stats)
    sums_out.wait_send()

    @pl.when(place + 1 < count)
    def _():
        for copy in upward:
            copy.wait_send()

    @pl.when(place > 0)
    def _():
        for copy in downward:
            copy.wait_send()

    forward(4, 0)
    forward(4, 1)
    swap_down.wait()
    swap_up.wait_send()
    for copy in out_a + out_b + out_c + list(flights.values()):
        copy.wait_send()


def state_mixer(
    value_rows,
    entry_rows,
    read_rows,
    gate_rows,
    steps,
    decay,
    index,
    value_taps,
    entry_taps,
    read_taps,
    gain,
    down,
    up,
    stream,
    out_weight,
    mixer_gain,
):
    height, value_width = value_rows.shape
    state_width = entry_rows.shape[1]
    groups, pairs, _ = steps.shape
    heads = pairs // 2
    wide = heads * HEAD_DIM
    blocks = height // BLOCK
    depth = lax.axis_size("sp") // 4
    edge = 16
    dma = pltpu.SemaphoreType.DMA
    vmem, anywhere = pl.BlockSpec(memory_space=pltpu.VMEM), pl.BlockSpec(memory_space=pl.ANY)
    return pl.pallas_call(
        states_kernel,
        out_shape=(
            jax.ShapeDtypeStruct((height, value_width), bf16),
            jax.ShapeDtypeStruct((down.shape[0], down.shape[1] // 2), bf16),
            jax.ShapeDtypeStruct((4 * depth, up.shape[0], up.shape[1] // 2), bf16),
        ),
        in_specs=[anywhere] * 4 + [vmem] * 7 + [anywhere] * 4 + [vmem],
        out_specs=(vmem, anywhere, anywhere),
        scratch_shapes=[
            pltpu.VMEM((height, value_width), bf16),
            pltpu.VMEM((height, state_width), bf16),
            pltpu.VMEM((height, state_width), bf16),
            pltpu.VMEM((height, value_width), bf16),
            pltpu.VMEM(stream.shape, bf16),
            pltpu.VMEM(out_weight.shape, bf16),
            pltpu.VMEM((height, value_width), bf16),
            pltpu.VMEM((height, value_width), bf16),
            pltpu.VMEM((height, 128), f32),
            pltpu.VMEM((height, 128), f32),
            pltpu.VMEM((blocks, 8, BLOCK), f32),
            pltpu.VMEM((height, BLOCK), f32),
            pltpu.VMEM((height + 16, wide), f32),
            pltpu.VMEM((edge, value_width), bf16),
            pltpu.VMEM((edge, state_width), bf16),
            pltpu.VMEM((edge, state_width), bf16),
            pltpu.VMEM((edge, value_width), bf16),
            pltpu.VMEM((edge, state_width), bf16),
            pltpu.VMEM((edge, state_width), bf16),
            pltpu.VMEM((height, value_width), bf16),
            pltpu.VMEM((height, state_width), bf16),
            pltpu.VMEM((height, state_width), bf16),
            pltpu.VMEM((groups, blocks, 2, wide, STATE), f32),
            pltpu.VMEM((groups, blocks, 4 * heads, BLOCK), f32),
            pltpu.VMEM((groups, blocks, BLOCK, BLOCK), f32),
            pltpu.VMEM((groups, blocks, pairs, BLOCK), f32),
            pltpu.VMEM((height, value_width), f32),
            pltpu.VMEM((blocks, 2, wide, STATE), bf16),
            pltpu.VMEM((groups, 2, wide, STATE), bf16),
            pltpu.VMEM((groups, pairs, BLOCK), f32),
            pltpu.VMEM((3, 2, wide, STATE), bf16),
            pltpu.VMEM((3, pairs, BLOCK), f32),
            pltpu.VMEM((2, wide, STATE), bf16),
            pltpu.VMEM((pairs, BLOCK), f32),
            pltpu.VMEM((depth - 1, wide, STATE), bf16),
            pltpu.VMEM((depth - 1, pairs, BLOCK), f32),
            pltpu.VMEM((4, 2, wide, STATE), bf16),
            pltpu.VMEM((3, 2, wide, STATE), bf16),
            dma((4, 3)),
            dma((4, 3)),
            dma((4, depth - 1)),
            dma((2, 3)),
            dma((4,)),
            dma((2, 2 * depth)),
            dma((2, 2 * depth)),
            dma((6,)),
            dma((4,)),
        ],
        compiler_params=pltpu.CompilerParams(
            collective_id=1, has_side_effects=True, vmem_limit_bytes=56 * 1024 * 1024
        ),
        cost_estimate=pl.CostEstimate(
            flops=60000000000, bytes_accessed=20000000, transcendentals=0
        ),
    )(
        value_rows,
        entry_rows,
        read_rows,
        gate_rows,
        steps,
        decay,
        index,
        value_taps,
        entry_taps,
        read_taps,
        gain,
        down,
        up,
        stream,
        out_weight,
        mixer_gain,
    )


def plain_states(
    head_value_rows,
    entry_map_rows,
    readout_map_rows,
    output_gate_rows,
    step_before_softplus,
    sudden_log_decay,
    document_index,
    head_rate_logarithm,
    head_step_bias,
    value_conv_taps,
    entry_conv_taps,
    readout_conv_taps,
    group_norm_gain,
):
    rows = head_value_rows.shape[0]
    heads = step_before_softplus.shape[1]
    groups = entry_map_rows.shape[1] // STATE
    per_group = heads // groups
    value_width = head_value_rows.shape[1]
    state_width = entry_map_rows.shape[1]
    blocks = rows // BLOCK
    sp_count = lax.axis_size("sp")
    place = lax.axis_index("sp")
    position = place * rows

    taps = value_conv_taps.shape[0]
    half = taps // 2
    ends = jnp.concatenate(
        [
            jnp.concatenate([a[rows - half :], a[:half]], axis=0)
            for a in (head_value_rows, entry_map_rows, readout_map_rows)
        ],
        axis=1,
    )
    low_all = shifted(ends[:half], 1)
    high_all = shifted(ends[half:], -1)
    doc_pad = jnp.pad(document_index, half + 1, constant_values=-1)
    window_ids = lax.dynamic_slice_in_dim(doc_pad, position + 1, rows + 2 * half)
    own_ids = window_ids[half : half + rows]
    prev_id = window_ids[half - 1]
    next_id = window_ids[half + rows]

    def conv(array, weights, start):
        width = array.shape[1]
        extended = jnp.concatenate(
            [low_all[:, start : start + width], array, high_all[:, start : start + width]], axis=0
        )
        weights = weights.astype(f32)
        total = weights[half] * array.astype(f32)
        for offset in range(taps):
            if offset == half:
                continue
            same = (window_ids[offset : offset + rows] == own_ids)[:, None]
            total = total + weights[offset] * jnp.where(
                same, extended[offset : offset + rows].astype(f32), 0.0
            )
        return jax.nn.silu(total).astype(bf16)

    values = conv(head_value_rows, value_conv_taps, 0)
    entries = conv(entry_map_rows, entry_conv_taps, value_width)
    readout = conv(readout_map_rows, readout_conv_taps, value_width + state_width)
    values = values.reshape(blocks, BLOCK, groups, per_group, HEAD_DIM)
    entries = entries.reshape(blocks, BLOCK, groups, STATE)
    readout = readout.reshape(blocks, BLOCK, groups, STATE)

    raw = step_before_softplus.astype(f32).T
    steps = jax.nn.softplus(raw[None] + head_step_bias[:, :, None])
    decay = -jnp.exp(head_rate_logarithm)[:, :, None] * steps + sudden_log_decay.T[None]
    shape = (2, groups, per_group, blocks, BLOCK)
    steps = jnp.transpose(steps.reshape(shape), (0, 3, 1, 2, 4))
    decay = jnp.transpose(decay.reshape(shape), (0, 3, 1, 2, 4))
    at = lax.iota(jnp.int32, BLOCK)
    upto = (at[:, None] <= at[None, :]).astype(f32)
    running = jnp.einsum("kbgrs,st->kbgrt", decay, upto, precision=exact_prec)
    totals = running[..., -1]
    ahead = running[0]
    behind = running[1] - decay[1]

    ids = own_ids.reshape(blocks, BLOCK)
    first_ids, last_ids = ids[:, 0], ids[:, -1]
    before = jnp.concatenate([prev_id[None], last_ids[:-1]])
    after = jnp.concatenate([first_ids[1:], next_id[None]])
    pass_f = jnp.where((before == last_ids)[:, None, None], jnp.exp(totals[0]), 0.0)
    pass_b = jnp.where((after == first_ids)[:, None, None], jnp.exp(totals[1]), 0.0)
    end_f = jnp.where(
        (ids == last_ids[:, None])[:, None, None], jnp.exp(totals[0][..., None] - ahead), 0.0
    ) * steps[0]
    end_b = jnp.where((ids == first_ids[:, None])[:, None, None], jnp.exp(behind), 0.0) * steps[1]
    arrive_f = jnp.where((ids == before[:, None])[:, None, None], jnp.exp(ahead), 0.0)
    arrive_b = jnp.where(
        (ids == after[:, None])[:, None, None], jnp.exp(totals[1][..., None] - behind), 0.0
    )

    own_f, own_b = jnp.prod(pass_f, axis=0), jnp.prod(pass_b, axis=0)

    def fresh_states(weight):
        weighted = values.astype(f32) * jnp.transpose(weight, (0, 3, 1, 2))[..., None]
        return jnp.einsum(
            "bsgrp,bsgn->bgrpn", weighted.astype(bf16), entries, preferred_element_type=f32
        )

    fresh_f = fresh_states(end_f)
    fresh_b = fresh_states(end_b)

    end_state = fresh_f[0]
    for b in range(1, blocks):
        end_state = end_state * pass_f[b][..., None, None] + fresh_f[b]
    start_state = fresh_b[blocks - 1]
    for b in range(blocks - 2, -1, -1):
        start_state = start_state * pass_b[b][..., None, None] + fresh_b[b]
    reach = -(-LONGEST_DOCUMENT // rows)
    in_f = incoming_state(end_state, own_f, 1, reach)
    in_b = incoming_state(start_state, own_b, -1, reach)

    scores = jnp.einsum("btgn,bsgn->bgts", readout, entries, preferred_element_type=f32)
    later = at[:, None] > at[None, :]
    equal = at[:, None] == at[None, :]
    linked = (ids[:, :, None] == ids[:, None, :])[:, None, None]
    spread = jnp.where(
        later,
        ahead[..., :, None] - ahead[..., None, :],
        behind[..., None, :] - behind[..., :, None],
    )
    strength = jnp.where(
        later,
        steps[0][..., None, :],
        jnp.where(equal, steps[0][..., None, :], 0.0) + steps[1][..., None, :],
    )
    weights = jnp.where(linked, jnp.exp(spread) * strength, 0.0)
    mixing = (scores[:, :, None] * weights).astype(bf16)
    output = jnp.einsum("bgrts,bsgrp->bgrtp", mixing, values, preferred_element_type=f32)

    state_f = [in_f]
    for b in range(blocks - 1):
        state_f.append(state_f[-1] * pass_f[b][..., None, None] + fresh_f[b])
    state_b = [in_b]
    for b in range(blocks - 1, 0, -1):
        state_b.append(state_b[-1] * pass_b[b][..., None, None] + fresh_b[b])
    entering_f = jnp.stack([s.astype(bf16) for s in state_f])
    entering_b = jnp.stack([s.astype(bf16) for s in state_b[::-1]])
    carried_f = jnp.einsum("btgn,bgrpn->bgrtp", readout, entering_f, preferred_element_type=f32)
    carried_b = jnp.einsum("btgn,bgrpn->bgrtp", readout, entering_b, preferred_element_type=f32)
    output = output + carried_f * arrive_f[..., None] + carried_b * arrive_b[..., None]

    gated = jnp.transpose(output, (0, 3, 1, 2, 4)).reshape(rows, groups, per_group * HEAD_DIM)
    gated = gated * jax.nn.silu(output_gate_rows.astype(f32)).reshape(gated.shape)
    gated = gated * lax.rsqrt(jnp.mean(gated * gated, axis=2, keepdims=True) + norm_eps)
    normed = (gated.reshape(rows, value_width) * group_norm_gain).astype(bf16)
    return normed


def ring_states(
    head_value_rows,
    entry_map_rows,
    readout_map_rows,
    output_gate_rows,
    step_before_softplus,
    sudden_log_decay,
    document_index,
    head_rate_logarithm,
    head_step_bias,
    value_conv_taps,
    entry_conv_taps,
    readout_conv_taps,
    group_norm_gain,
    *dense,
):
    rows = head_value_rows.shape[0]
    heads = step_before_softplus.shape[1]
    groups = entry_map_rows.shape[1] // STATE
    raw = step_before_softplus.astype(f32).T
    steps = jax.nn.softplus(raw[None] + head_step_bias[:, :, None])
    decay = -jnp.exp(head_rate_logarithm)[:, :, None] * steps + sudden_log_decay.T[None]

    def by_group(array):
        array = array.reshape(2, groups, heads // groups, rows)
        return jnp.transpose(array, (1, 0, 2, 3)).reshape(groups, -1, rows)

    return state_mixer(
        head_value_rows,
        entry_map_rows,
        readout_map_rows,
        output_gate_rows,
        by_group(steps),
        by_group(decay),
        document_index.reshape(-1, BLOCK),
        value_conv_taps,
        entry_conv_taps,
        readout_conv_taps,
        group_norm_gain[None],
        *dense,
    )


def per_device(
    head_value_rows,
    entry_map_rows,
    readout_map_rows,
    output_gate_rows,
    step_before_softplus,
    sudden_log_decay,
    document_index,
    head_rate_logarithm,
    head_step_bias,
    value_conv_taps,
    entry_conv_taps,
    readout_conv_taps,
    group_norm_gain,
    mixer_output_weight,
    stream,
    mixer_norm_gain,
    channel_norm_gain,
    up_projection_weight,
    down_projection_weight,
):
    model_width = mixer_output_weight.shape[1]
    rows = head_value_rows.shape[0]
    inputs = (
        head_value_rows,
        entry_map_rows,
        readout_map_rows,
        output_gate_rows,
        step_before_softplus,
        sudden_log_decay,
        document_index,
        head_rate_logarithm,
        head_step_bias,
        value_conv_taps,
        entry_conv_taps,
        readout_conv_taps,
        group_norm_gain,
    )
    if has_rings() and entry_map_rows.shape[1] == 4 * STATE:
        normed_one, other, up_all = ring_states(
            *inputs,
            down_projection_weight,
            up_projection_weight,
            stream,
            mixer_output_weight,
            mixer_norm_gain[None],
        )
        return ring_mixer(
            normed_one,
            channel_norm_gain[None],
            down_projection_weight,
            other,
            up_projection_weight,
            up_all,
        )
    up_half, down_half = pair_weights(up_projection_weight), pair_weights(down_projection_weight)
    normed = plain_states(*inputs)
    mixer_sum = tp_scatter(jnp.dot(normed, mixer_output_weight, preferred_element_type=f32))
    first_sum = resid_scale * stream.astype(f32) + mixer_sum
    normed_one = norm_rows(first_sum, mixer_norm_gain, model_width)
    piece = rows // PIECES
    returned = [
        pair_swap(
            channel_mixer(
                pair_swap(normed_one[i * piece : (i + 1) * piece]),
                up_half,
                down_half,
            ).astype(bf16)
        )
        for i in range(PIECES)
    ]
    down_sum = channel_mixer(normed_one, up_half, down_half) + jnp.concatenate(returned).astype(f32)
    second_sum = resid_scale * normed_one.astype(f32) + down_sum
    return norm_rows(second_sum, channel_norm_gain, model_width)


def solution(mesh):
    placed = (
        P("sp", "tp"),
        P("sp", "tp"),
        P("sp", "tp"),
        P("sp", "tp"),
        P("sp", "tp"),
        P("sp", "tp"),
        P(),
        P(None, "tp"),
        P(None, "tp"),
        P(None, "tp"),
        P(None, "tp"),
        P(None, "tp"),
        P("tp"),
        P("tp", None),
        P("sp", "tp"),
        P("tp"),
        P("tp"),
        P("sp", "tp"),
        P("sp", "tp"),
    )
    return jax.shard_map(
        per_device, mesh=mesh, in_specs=placed, out_specs=P("sp", "tp"), check_vma=False
    )
```

```python
import jax
import jax.numpy as jnp
from jax import lax
from jax.experimental import pallas as pl
from jax.experimental.pallas import tpu as pltpu
from jax.sharding import PartitionSpec as P

HEAD_DIM = 64
STATE = 128
BLOCK = 128
LONGEST_DOCUMENT = 6144
PIECES = 2


exact_prec = lax.Precision.HIGHEST
norm_eps = 1e-05
resid_scale = 1.4142135623730951
bf16 = jnp.bfloat16
f32 = jnp.float32


def swap(array):
    return lax.ppermute(array, "tp", [(0, 1), (1, 0)])


def tp_scatter(partial):
    if lax.axis_size("tp") != 2:
        return lax.psum_scatter(
            partial.astype(bf16), "tp", scatter_dimension=1, tiled=True
        ).astype(f32)
    me = lax.axis_index("tp")
    width = partial.shape[1] // 2
    rounded = partial.astype(bf16)
    other = lax.dynamic_slice_in_dim(rounded, (1 - me) * width, width, 1)
    mine = lax.dynamic_slice_in_dim(rounded, me * width, width, 1)
    return mine.astype(f32) + swap(other).astype(f32)


def tp_gather(array):
    if lax.axis_size("tp") != 2:
        return lax.all_gather(array, "tp", axis=1, tiled=True)
    other = swap(array)
    first = lax.axis_index("tp") == 0
    return jnp.concatenate(
        [jnp.where(first, array, other), jnp.where(first, other, array)], axis=1
    )


def norm_rows(residual, gain, width):
    sums = jnp.stack([jnp.sum(residual, axis=1), jnp.sum(residual * residual, axis=1)])
    if lax.axis_size("tp") == 2:
        sums = sums + swap(sums)
    else:
        sums = lax.psum(sums, "tp")
    row_mean = sums[0] / width
    row_var = sums[1] / width - row_mean * row_mean
    return ((residual - row_mean[:, None]) * lax.rsqrt(row_var + norm_eps)[:, None] * gain).astype(
        bf16
    )


def pair_swap(array, bit=1):
    count = lax.axis_size("sp")
    return lax.ppermute(array, "sp", [(i, i ^ bit) for i in range(count)])


def pair_weights(weight):
    count = lax.axis_size("sp")
    odd = lax.axis_index("sp") % 2
    width = weight.shape[1] // 2
    mine = lax.dynamic_slice_in_dim(weight, odd * width, width, 1)
    other = pair_swap(lax.dynamic_slice_in_dim(weight, (1 - odd) * width, width, 1))
    both = jnp.concatenate(
        [jnp.where(odd == 0, mine, other), jnp.where(odd == 0, other, mine)], axis=0
    )
    members = [list(range(0, count, 2)), list(range(1, count, 2))]
    return lax.all_gather(both, "sp", axis=0, tiled=True, axis_index_groups=members)


def has_rings():
    return lax.axis_size("tp") == 2 and lax.axis_size("sp") == 2 * RING


MESH_ID = pl.DeviceIdType.MESH
RING = 8


def ring_place(spot, depth):
    far = spot // depth
    return spot + far * (2 * depth - 1 - 2 * spot), far


def ring_flights(remote, size, after, before, store, first, send, recv):
    flights = {}
    for direction, to in enumerate((after, before)):
        for distance in range(size // 2):
            for part in (0, 1):
                if distance == size // 2 - 1 and part != direction:
                    continue
                here = (size - distance) % size if direction == 0 else distance
                there = (here + size - 1) % size if direction == 0 else here + 1
                n = 2 * distance + part
                flights[direction, distance, part] = remote(
                    first[part] if distance == 0 else store.at[2 * here + part],
                    store.at[2 * there + part],
                    send.at[direction, n],
                    recv.at[direction, n],
                    to,
                )
    return flights


def pass_on(flights, distance, turn, flip):
    for direction in (0, 1):
        part = 1 - turn if flip and direction else turn
        if (direction, distance - 1, part) in flights:
            flights[direction, distance - 1, part].wait_recv()
        if (direction, distance, part) in flights:
            flights[direction, distance, part].start()


def twin_norm(remote, twin, sums, gain_ref, store, send_s, recv_s, sems):
    height, width = sums.shape
    cut = 128
    lane = lax.broadcasted_iota(jnp.int32, (cut, 128), 1)
    for i in range(height // cut):
        value = sums[pl.ds(i * cut, cut), :]
        total = jnp.sum(value, axis=1, keepdims=True)
        power = jnp.sum(value * value, axis=1, keepdims=True)
        send_s[pl.ds(i * cut, cut), :] = jnp.where(lane == 0, total, power)
    stats_out = remote(send_s, recv_s, sems.at[0], sems.at[1], twin)
    stats_out.start()
    stats_out.wait_recv()
    for i in range(height // cut):
        at = pl.ds(i * cut, cut)
        stats = (send_s[at, :] + recv_s[at, :]) / (2 * width)
        mean = stats[:, 0:1]
        scale = lax.rsqrt(stats[:, 1:2] - mean * mean + norm_eps)
        store(at, ((sums[at, :] - mean) * scale * gain_ref[...]).astype(bf16))
    stats_out.wait_send()


def mixer_kernel(
    rows_ref,
    gain_ref,
    down_ref,
    other_ref,
    up_ref,
    up_all_ref,
    out_ref,
    sum_ref,
    send_s,
    recv_s,
    down,
    up,
    rows,
    squared,
    local,
    send_t,
    recv_t,
    keep_o,
    keep_x,
    send_x,
    recv_x,
    up_sem,
    own_sem,
    row_send,
    row_recv,
    ring_send,
    ring_recv,
    t_sems,
    x_sems,
    first_sems,
):
    count = lax.axis_size("sp")
    depth = count // 4
    size = count // 2
    place = lax.axis_index("sp")
    me = lax.axis_index("tp")
    z, y, x = place // 4, (place // 2) % 2, place % 2
    spot = z + y * (2 * depth - 1 - 2 * z)
    height, width = rows_ref.shape
    half = height // 2
    hidden_width = up.shape[1]
    piece = down.shape[1]
    tile = 2 * piece
    mine = pl.ds(pl.multiple_of(x * hidden_width, hidden_width), hidden_width)

    def member(where):
        level, far = ring_place(where, depth)
        return level * 4 + far * 2 + x

    after = (member((spot + 1) % size), me)
    before = (member((spot + size - 1) % size), me)
    across = place + 1 - 2 * x
    twin = (place, 1 - me)
    opposite = (across, me)

    barrier = pltpu.get_barrier_semaphore()
    near = (after, before, twin, opposite)
    for device in near:
        pl.semaphore_signal(barrier, inc=1, device_id=device, device_id_type=MESH_ID)
    pl.semaphore_wait(barrier, len(near))

    def remote(source, target, send, recv, device):
        return pltpu.make_async_remote_copy(
            src_ref=source,
            dst_ref=target,
            send_sem=send,
            recv_sem=recv,
            device_id=device,
            device_id_type=MESH_ID,
        )

    pending = []

    first = (down_ref.at[:, mine], other_ref)
    flights = ring_flights(remote, size, after, before, down, first, ring_send, ring_recv)
    pending.extend(flights.values())
    for direction in (0, 1):
        for part in (0, 1) if direction == 0 else (1, 0):
            flights[direction, 0, part].start()

    def forward(distance, turn):
        pass_on(flights, distance, turn, True)

    loads = []
    for i in range(size):
        base = member((spot + i) % size)
        for part, source in enumerate((base, base + 1 - 2 * x)):
            loads.append(
                pltpu.make_async_copy(
                    up_ref.at[:, mine] if i + part == 0 else up_all_ref.at[2 * i + part],
                    up.at[pl.ds(pl.multiple_of(source * piece, piece), piece)],
                    up_sem.at[2 * i + part],
                )
            )
    own = [
        pltpu.make_async_copy(down_ref.at[:, mine], down.at[0], own_sem.at[0]),
        pltpu.make_async_copy(other_ref, down.at[1], own_sem.at[1]),
    ]
    my_columns = pl.ds(pl.multiple_of(me * width, width), width)
    parts = [pl.ds(i * half, half) for i in range(4)]
    to_twin = remote(
        rows_ref, rows.at[pl.ds(0, height), my_columns], row_send.at[0], row_recv.at[0], twin
    )
    outward = [
        remote(
            rows_ref.at[parts[i]],
            rows.at[parts[2 + i], my_columns],
            row_send.at[1 + i],
            row_recv.at[1 + i],
            opposite,
        )
        for i in range(2)
    ]
    inward = [
        remote(
            rows.at[parts[2 + i], my_columns],
            rows.at[parts[2 + i], my_columns],
            row_send.at[3 + i],
            row_recv.at[3 + i],
            twin,
        )
        for i in range(2)
    ]
    for copy in [to_twin] + outward:
        copy.start()
    pending.extend([to_twin] + outward + inward)
    for copy in loads + own:
        copy.start()
    rows[pl.ds(0, height), my_columns] = rows_ref[...]

    to_twin.wait_recv()
    for copy in loads:
        copy.wait()

    def raise_rows(start, length):
        def body(i, carry):
            columns = pl.ds(pl.multiple_of(i * tile, tile), tile)
            value = jnp.dot(
                rows[pl.ds(start, length), :], up[:, columns], preferred_element_type=f32
            )
            value = jnp.maximum(value, 0.0)
            squared[pl.ds(start, length), columns] = (value * value).astype(bf16)
            return carry

        lax.fori_loop(0, hidden_width // tile, body, 0)

    raise_rows(0, height)
    forward(1, 0)
    outward[0].wait_recv()
    inward[0].start()
    forward(1, 1)
    inward[0].wait_recv()
    raise_rows(height, half)
    forward(2, 0)
    outward[1].wait_recv()
    inward[1].start()
    inward[1].wait_recv()
    raise_rows(height + half, half)
    for copy in own:
        copy.wait()

    def owner(where):
        level, _ = ring_place(where, depth)
        return level // (depth // 2)

    def product(slot, start):
        return lax.dot_general(
            squared[pl.ds(start, height), :],
            down[pl.ds(2 * slot, 2)].reshape(tile, hidden_width),
            (((1,), (1,)), ((), ())),
            preferred_element_type=f32,
        )

    spare = size // 2
    handed = [
        remote(
            send_t.at[2 * (i % spare) + part],
            recv_t.at[2 * (i % spare) + part],
            t_sems.at[0, 2 * (i % spare) + part],
            t_sems.at[1, 2 * (i % spare) + part],
            twin,
        )
        for i in range(size)
        for part in (0, 1)
    ]
    returned = [
        remote(
            send_x.at[i % spare],
            recv_x.at[i % spare],
            x_sems.at[0, i % spare],
            x_sems.at[1, i % spare],
            opposite,
        )
        for i in range(size)
    ]
    is_ours = [owner((spot + i) % size) == me for i in range(size)]
    is_theirs = [owner((spot + i) % size) != me for i in range(size)]

    def lower(i):
        k = i % spare
        keep_x[...] = product(i, height)

        @pl.when(is_theirs[i])
        def _():
            send_t[2 * k] = keep_x[...].astype(bf16)
            handed[2 * i].start()

        keep_o[...] = product(i, 0).astype(bf16)

        @pl.when(is_ours[i])
        def _():
            local[k] = keep_o[...]
            handed[2 * i].wait_recv()
            send_x[k] = (keep_x[...] + recv_t[2 * k].astype(f32)).astype(bf16)
            returned[i].start()

        @pl.when(is_theirs[i])
        def _():
            send_t[2 * k + 1] = keep_o[...]
            handed[2 * i + 1].start()

    sum_ref[...] = resid_scale * rows_ref[...].astype(f32)

    def settle(i):
        k = i % spare

        @pl.when(is_ours[i])
        def _():
            base = member((spot + i) % size) - me * (count // 2)
            pair = base + 1 - 2 * x
            handed[2 * i + 1].wait_recv()
            returned[i].wait_recv()
            for part, spot_at in enumerate((base, pair)):
                columns = pl.ds(part * piece, piece)
                swapped = pl.ds((1 - part) * piece, piece)
                target = pl.ds(pl.multiple_of(spot_at * piece, piece), piece)
                sum_ref[:, target] += (
                    local[k, :, columns].astype(f32)
                    + recv_t[2 * k + 1, :, columns].astype(f32)
                    + recv_x[k, :, swapped].astype(f32)
                )

    lower(0)
    lower(1)
    lower(size - 1)
    forward(2, 1)
    lower(2)
    lower(size - 2)
    forward(3, 0)
    settle(0)
    settle(1)
    settle(size - 1)
    forward(3, 1)
    lower(3)
    lower(size - 3)
    settle(2)
    settle(size - 2)
    forward(4, 0)
    lower(4)
    settle(3)
    settle(size - 3)
    settle(4)

    def store_out(at, value):
        out_ref[at, :] = value

    twin_norm(remote, twin, sum_ref, gain_ref, store_out, send_s, recv_s, first_sems)
    for copy in pending:
        copy.wait_send()
    for i in range(size):

        @pl.when(is_theirs[i])
        def _(i=i):
            handed[2 * i].wait_send()
            handed[2 * i + 1].wait_send()

        @pl.when(is_ours[i])
        def _(i=i):
            returned[i].wait_send()


def ring_mixer(rows, gain, down, other, up, up_all):
    count = lax.axis_size("sp")
    height, width = rows.shape
    size = count // 2
    piece, hidden = other.shape
    tile, spare = 2 * piece, size // 2
    dma = pltpu.SemaphoreType.DMA
    vmem, anywhere = pl.BlockSpec(memory_space=pltpu.VMEM), pl.BlockSpec(memory_space=pl.ANY)
    return pl.pallas_call(
        mixer_kernel,
        out_shape=jax.ShapeDtypeStruct((height, width), bf16),
        in_specs=[vmem, vmem] + [anywhere] * 4,
        out_specs=vmem,
        scratch_shapes=[
            pltpu.VMEM((height, width), f32),
            pltpu.VMEM((height, 128), f32),
            pltpu.VMEM((height, 128), f32),
            pltpu.VMEM((count, piece, hidden), bf16),
            pltpu.VMEM((2 * width, hidden), bf16),
            pltpu.VMEM((2 * height, 2 * width), bf16),
            pltpu.VMEM((2 * height, hidden), bf16),
            pltpu.VMEM((spare, height, tile), bf16),
            pltpu.VMEM((2 * spare, height, tile), bf16),
            pltpu.VMEM((2 * spare, height, tile), bf16),
            pltpu.VMEM((height, tile), bf16),
            pltpu.VMEM((height, tile), f32),
            pltpu.VMEM((spare, height, tile), bf16),
            pltpu.VMEM((spare, height, tile), bf16),
            dma((count,)),
            dma((2,)),
            dma((5,)),
            dma((5,)),
            dma((2, size)),
            dma((2, size)),
            dma((2, 2 * spare)),
            dma((2, spare)),
            dma((2,)),
        ],
        compiler_params=pltpu.CompilerParams(
            collective_id=0, has_side_effects=True, vmem_limit_bytes=62 * 1024 * 1024
        ),
        cost_estimate=pl.CostEstimate(
            flops=8 * height * 2 * width * hidden, bytes_accessed=30000000, transcendentals=0
        ),
    )(rows, gain, down, other, up, up_all)


def channel_mixer(rows, up, down):
    hidden = jnp.dot(tp_gather(rows), up, preferred_element_type=f32)
    squared = jnp.square(jax.nn.relu(hidden)).astype(bf16)
    part = lax.dot_general(squared, down, (((1,), (1,)), ((), ())), preferred_element_type=f32)
    return tp_scatter(part)


def shifted(array, step):
    count = lax.axis_size("sp")
    if step > 0:
        pairs = [(i, i + step) for i in range(count - step)]
    else:
        pairs = [(i, i + step) for i in range(-step, count)]
    return lax.ppermute(array, "sp", pairs)


def with_decay(state, through):
    heads = through.size
    flat = state.reshape(heads, -1).astype(bf16)
    through = through.reshape(heads, 1)
    high = through.astype(bf16)
    middle = (through - high.astype(f32)).astype(bf16)
    low = (through - high.astype(f32) - middle.astype(f32)).astype(bf16)
    terms = jnp.concatenate([high, middle, low], axis=1)
    return jnp.concatenate([flat, jnp.pad(terms, ((0, 0), (0, 125)))], axis=1)


def apart(packed, shape):
    terms = packed[:, -128:].astype(f32)
    through = terms[:, 0] + (terms[:, 1] + terms[:, 2])
    return packed[:, :-128].astype(f32).reshape(shape), through.reshape(shape[:2])


def incoming_state(end_state, own_pass, direction, reach):
    count = lax.axis_size("sp")
    shape = end_state.shape
    state, through = apart(shifted(with_decay(end_state, own_pass), direction), shape)
    covered = 1
    while covered < min(reach, count - 1):
        more, further = apart(shifted(with_decay(state, through), direction * covered), shape)
        state = state + through[..., None, None] * more
        through = through * further
        covered *= 2
    return state


def scaled(state, scale, heads):
    head_dim = state.shape[0] // heads
    return jnp.concatenate(
        [
            state[h * head_dim : (h + 1) * head_dim] * scale[h : h + 1, :]
            for h in range(heads)
        ],
        axis=0,
    )


def spread_heads(columns, first, heads, lane):
    parts = []
    for h in range(0, heads, 2):
        parts.append(
            jnp.where(
                lane, columns[:, first + h : first + h + 1], columns[:, first + h + 1 : first + h + 2]
            )
        )
    return jnp.concatenate(parts, axis=1)


def states_kernel(
    value_ref,
    entry_ref,
    read_ref,
    gate_ref,
    step_ref,
    sudden_ref,
    rate_ref,
    bias_ref,
    index_ref,
    value_taps,
    entry_taps,
    read_taps,
    gain_ref,
    down_ref,
    up_ref,
    stream_ref,
    out_weight_ref,
    mixer_gain_ref,
    out_ref,
    other_ref,
    up_all,
    value_in,
    entry_in,
    read_in,
    gate_in,
    stream_in,
    out_weight,
    normed,
    recv_o,
    send_s,
    recv_s,
    step_in,
    sudden_in,
    square,
    steps_ref,
    decay_ref,
    edges_ref,
    same_ref,
    ext,
    value_low,
    entry_low,
    read_low,
    value_high,
    entry_high,
    read_high,
    values,
    entries,
    reads,
    fresh,
    vectors,
    columns,
    passing,
    within,
    entering,
    send_a,
    decay_a,
    recv_a,
    table_a,
    send_b,
    decay_b,
    recv_b,
    table_b,
    send_c,
    recv_c,
    halo_sems,
    a_sems,
    b_sems,
    c_sems,
    swap_sems,
    ring_send,
    ring_recv,
    load_sems,
    first_sems,
):
    count = lax.axis_size("sp")
    place = lax.axis_index("sp")
    me = lax.axis_index("tp")
    depth = count // 4
    z, q = place // 4, place % 4
    height = value_ref.shape[0]
    groups = entry_ref.shape[1] // STATE
    blocks = height // BLOCK
    heads = step_ref.shape[0] // groups
    wide = heads * HEAD_DIM
    edge = value_low.shape[0]

    plane = [(z * 4 + (q + i) % 4, me) for i in (1, 2, 3)]
    tower = [(((z + i) % depth) * 4 + q, me) for i in range(1, depth)]
    up_place, down_place = (place + 1, me), (place - 1, me)
    twin = (place, 1 - me)
    loads = [
        pltpu.make_async_copy(source, target, load_sems.at[i])
        for i, (source, target) in enumerate(
            (
                (value_ref, value_in),
                (entry_ref, entry_in),
                (read_ref, read_in),
                (gate_ref, gate_in),
                (stream_ref, stream_in),
                (out_weight_ref, out_weight),
                (step_ref, step_in),
                (sudden_ref, sudden_in),
            )
        )
    ]
    for copy in loads:
        copy.start()

    barrier = pltpu.get_barrier_semaphore()

    @pl.when(place + 1 < count)
    def _():
        pl.semaphore_signal(barrier, inc=1, device_id=up_place, device_id_type=MESH_ID)

    @pl.when(place > 0)
    def _():
        pl.semaphore_signal(barrier, inc=1, device_id=down_place, device_id_type=MESH_ID)

    for device in plane + tower + [twin]:
        pl.semaphore_signal(barrier, inc=1, device_id=device, device_id_type=MESH_ID)

    @pl.when((place > 0) & (place + 1 < count))
    def _():
        pl.semaphore_wait(barrier, len(plane) + len(tower) + 3)

    @pl.when((place == 0) | (place + 1 == count))
    def _():
        pl.semaphore_wait(barrier, len(plane) + len(tower) + 2)

    def remote(source, target, send, recv, device):
        return pltpu.make_async_remote_copy(
            src_ref=source,
            dst_ref=target,
            send_sem=send,
            recv_sem=recv,
            device_id=device,
            device_id_type=MESH_ID,
        )

    raw = (value_ref, entry_ref, read_ref)
    lows, highs = (value_low, entry_low, read_low), (value_high, entry_high, read_high)
    upward = [
        remote(
            raw[i].at[pl.ds(height - edge, edge)],
            lows[i],
            halo_sems.at[0, i],
            halo_sems.at[1, i],
            up_place,
        )
        for i in range(3)
    ]
    downward = [
        remote(
            raw[i].at[pl.ds(0, edge)], highs[i], halo_sems.at[2, i], halo_sems.at[3, i], down_place
        )
        for i in range(3)
    ]

    @pl.when(place + 1 < count)
    def _():
        for copy in upward:
            copy.start()

    @pl.when(place > 0)
    def _():
        for copy in downward:
            copy.start()

    x = place % 2
    share = other_ref.shape[1]
    mine = pl.ds(pl.multiple_of(x * share, share), share)
    theirs = pl.ds(pl.multiple_of((1 - x) * share, share), share)
    opposite = (place + 1 - 2 * x, me)
    swap_up = remote(
        up_ref.at[:, theirs], up_all.at[1], swap_sems.at[2], swap_sems.at[3], opposite
    )
    swap_down = remote(
        down_ref.at[:, theirs], other_ref, swap_sems.at[0], swap_sems.at[1], opposite
    )
    size = count // 2
    y = (place // 2) % 2
    spot = z + y * (2 * depth - 1 - 2 * z)

    def member(where):
        level, far = ring_place(where, depth)
        return level * 4 + far * 2 + x

    flights = ring_flights(
        remote,
        size,
        (member((spot + 1) % size), me),
        (member((spot + size - 1) % size), me),
        up_all,
        (up_ref.at[:, mine], up_all.at[1]),
        ring_send,
        ring_recv,
    )
    swap_up.start()
    for direction in (0, 1):
        flights[direction, 0, 0].start()
    swap_down.start()

    def forward(distance, turn):
        pass_on(flights, distance, turn, False)

    @pl.when(place == 0)
    def _():
        for low in lows:
            low[...] = jnp.zeros_like(low)

    @pl.when(place + 1 == count)
    def _():
        for high in highs:
            high[...] = jnp.zeros_like(high)

    @pl.when(place > 0)
    def _():
        for copy in upward:
            copy.wait_recv()

    @pl.when(place + 1 < count)
    def _():
        for copy in downward:
            copy.wait_recv()

    row_at = lax.broadcasted_iota(jnp.int32, (BLOCK, BLOCK), 0)
    lane_at = lax.broadcasted_iota(jnp.int32, (BLOCK, BLOCK), 1)
    later, earlier = row_at > lane_at, row_at < lane_at
    upto = (row_at <= lane_at).astype(f32)
    left_lane = lane_at < HEAD_DIM

    def conv(source, low, high, taps, target, at, width):
        ext[pl.ds(8, height), pl.ds(0, width)] = source[:, at].astype(f32)
        ext[pl.ds(0, 8), pl.ds(0, width)] = low[pl.ds(edge - 8, 8), at].astype(f32)
        ext[pl.ds(8 + height, 8), pl.ds(0, width)] = high[pl.ds(0, 8), at].astype(f32)
        weights = taps[:, at].astype(f32)
        for b in range(blocks):
            total = None
            for offset in range(5):
                piece = ext[pl.ds(b * BLOCK + 6 + offset, BLOCK), pl.ds(0, width)]
                if offset != 2:
                    piece = piece * same_ref[pl.ds(b * BLOCK, BLOCK), pl.ds(offset, 1)]
                piece = piece * weights[offset : offset + 1, :]
                total = piece if total is None else total + piece
            total = total / (1.0 + jnp.exp(-total))
            target[pl.ds(b * BLOCK, BLOCK), at] = total.astype(bf16)

    out_a = []
    for i in (1, 2, 3):
        target = (q + i) % 4
        out_a.append(
            remote(
                send_a.at[target],
                recv_a.at[i - 1],
                a_sems.at[0, i - 1],
                a_sems.at[1, i - 1],
                plane[i - 1],
            )
        )
        out_a.append(
            remote(
                decay_a.at[target],
                table_a.at[i - 1],
                a_sems.at[2, i - 1],
                a_sems.at[3, i - 1],
                plane[i - 1],
            )
        )

    def local_group(i, carry):
        g = (q + 1 + i) % groups
        at_wide = pl.ds(pl.multiple_of(g * wide, wide), wide)
        at_state = pl.ds(pl.multiple_of(g * STATE, STATE), STATE)
        conv(value_in, value_low, value_high, value_taps, values, at_wide, wide)
        conv(entry_in, entry_low, entry_high, entry_taps, entries, at_state, STATE)
        conv(read_in, read_low, read_high, read_taps, reads, at_state, STATE)
        whole = None
        ends = None
        for b in range(blocks):
            lanes = pl.ds(b * BLOCK, BLOCK)
            steps, decay = steps_ref[g, :, lanes], decay_ref[g, :, lanes]
            running = jnp.dot(
                decay, upto, precision=exact_prec, preferred_element_type=f32
            )
            totals = jnp.broadcast_to(running[:, BLOCK - 1 :], running.shape)
            ahead = running[:heads]
            behind = running[heads:] - decay[heads:]
            total_f, total_b = totals[:heads], totals[heads:]
            edges = edges_ref[b]
            ids, before, after = edges[0:1], edges[1:2], edges[2:3]
            first, last = edges[3:4], edges[4:5]

            def keep(one, two, value):
                one, two = jnp.broadcast_to(one, value.shape), jnp.broadcast_to(two, value.shape)
                return jnp.where(one == two, value, 0.0)

            pass_f = keep(before, last, jnp.exp(total_f))
            pass_b = keep(after, first, jnp.exp(total_b))
            end_f = keep(ids, last, jnp.exp(total_f - ahead)) * steps[:heads]
            end_b = keep(ids, first, jnp.exp(behind)) * steps[heads:]
            arrive_f = keep(ids, before, jnp.exp(ahead))
            arrive_b = keep(ids, after, jnp.exp(total_b - behind))
            passes = jnp.concatenate([pass_f, pass_b], axis=0)
            passing[g, b] = passes
            whole = passes if whole is None else whole * passes
            vectors[g, b] = jnp.concatenate([ahead, behind, steps], axis=0)
            tall = jnp.concatenate([ahead, behind, arrive_f, arrive_b, end_f, end_b], axis=0)
            tall = jnp.concatenate(
                [tall, jnp.zeros((BLOCK - tall.shape[0], BLOCK), f32)], axis=0
            )
            turned = jnp.transpose(tall)
            columns[g, b] = turned
            value = values[lanes, at_wide].astype(f32)
            entry = entries[lanes, at_state]
            both = []
            for k in range(2):
                weighted = value * spread_heads(turned, (4 + k) * heads, heads, left_lane)
                both.append(
                    lax.dot_general(
                        weighted.astype(bf16),
                        entry,
                        (((0,), (0,)), ((), ())),
                        preferred_element_type=f32,
                    )
                )
                fresh[g, b, k] = both[k]
            ends = both[0] if ends is None else scaled(ends, pass_f, heads) + both[0]
        send_a[g, 0] = ends.astype(bf16)
        starts = fresh[g, blocks - 1, 1]
        for b in range(blocks - 2, -1, -1):
            starts = scaled(starts, passing[g, b][heads:], heads) + fresh[g, b, 1]
        send_a[g, 1] = starts.astype(bf16)
        decay_a[g] = whole

        for k in range(groups - 1):

            @pl.when(i == k)
            def _(k=k):
                out_a[2 * k].start()
                out_a[2 * k + 1].start()

        @pl.when(i == 0)
        def _():
            swap_up.wait_recv()
            for direction in (0, 1):
                flights[direction, 0, 1].start()
            forward(1, 0)

        @pl.when(i == 2)
        def _():
            forward(1, 1)

        return carry

    def index_row(b):
        at = jnp.clip(place * blocks + b, 0, count * blocks - 1)
        row = index_ref[pl.ds(at, 1), :].astype(f32)
        outside = (place * blocks + b < 0) | (place * blocks + b >= count * blocks)
        return jnp.where(outside, jnp.full_like(row, -1.0), row)

    index_rows = [index_row(b) for b in range(-1, blocks + 1)]
    for b in range(blocks):
        prior, row, following = index_rows[b : b + 3]
        line = row.shape
        first = jnp.broadcast_to(row[:, :1], line)
        last = jnp.broadcast_to(row[:, BLOCK - 1 :], line)
        before = jnp.broadcast_to(prior[:, BLOCK - 1 :], line)
        after = jnp.broadcast_to(following[:, :1], line)
        edges_ref[b] = jnp.concatenate([row, before, after, first, last] + [row] * 3, axis=0)
        long = jnp.concatenate([prior, row, following], axis=1)
        moved = [long[:, BLOCK + o - 2 : 2 * BLOCK + o - 2] for o in range(5)]
        flags = [jnp.where(m == row, 1.0, 0.0) for m in moved] + [row]
        zeros = jnp.zeros((BLOCK - len(flags), BLOCK), f32)
        same_ref[pl.ds(b * BLOCK, BLOCK), :] = jnp.transpose(
            jnp.concatenate(flags + [zeros], axis=0)
        )
    for copy in loads[:3] + loads[6:]:
        copy.wait()

    every = groups * heads
    square[...] = jnp.zeros_like(square)
    square[pl.ds(0, 2), pl.ds(0, every)] = bias_ref[...]
    square[pl.ds(2, 2), pl.ds(0, every)] = rate_ref[...]
    settings = jnp.transpose(square[...])[:every]
    for b in range(blocks):
        lanes = pl.ds(b * BLOCK, BLOCK)
        lengths, decays = [], []
        for k in range(2):
            before_softplus = step_in[:, lanes].astype(f32) + settings[:, k : k + 1]
            length = jnp.maximum(before_softplus, 0.0) + jnp.log1p(
                jnp.exp(-jnp.abs(before_softplus))
            )
            lengths.append(length)
            decays.append(
                sudden_in[:, lanes] - jnp.exp(settings[:, 2 + k : 3 + k]) * length
            )
        for g in range(groups):
            span = slice(g * heads, (g + 1) * heads)
            steps_ref[g, :, lanes] = jnp.concatenate([v[span] for v in lengths], axis=0)
            decay_ref[g, :, lanes] = jnp.concatenate([v[span] for v in decays], axis=0)
    lax.fori_loop(0, groups, local_group, 0)

    def diagonal(i, carry):
        g, b = i // blocks, i % blocks
        at_wide = pl.ds(pl.multiple_of(g * wide, wide), wide)
        at_state = pl.ds(pl.multiple_of(g * STATE, STATE), STATE)
        at_rows = pl.ds(pl.multiple_of(b * BLOCK, BLOCK), BLOCK)
        score = lax.dot_general(
            reads[at_rows, at_state],
            entries[at_rows, at_state],
            (((1,), (1,)), ((), ())),
            preferred_element_type=f32,
        )
        edges = edges_ref[b]
        score = jnp.where(same_ref[at_rows, 5:6] == edges[0:1], score, 0.0)
        turned, vector = columns[g, b], vectors[g, b]
        value = values[at_rows, at_wide]
        lane = lax.broadcasted_iota(jnp.int32, value.shape, 1) // HEAD_DIM
        total = None
        for h in range(heads):
            spread = jnp.where(
                later,
                turned[:, h : h + 1] - vector[h : h + 1, :],
                vector[heads + h : heads + h + 1, :] - turned[:, heads + h : heads + h + 1],
            )
            strength = jnp.where(earlier, 0.0, vector[2 * heads + h : 2 * heads + h + 1, :])
            strength = strength + jnp.where(
                later, 0.0, vector[3 * heads + h : 3 * heads + h + 1, :]
            )
            mixing = (score * (jnp.exp(spread) * strength)).astype(bf16)
            masked = jnp.where(lane == h, value, jnp.zeros_like(value))
            part = jnp.dot(mixing, masked, preferred_element_type=f32)
            total = part if total is None else total + part
        within[at_rows, at_wide] = total
        return carry

    for copy in out_a:
        copy.wait_recv()

    def slot_of(member):
        return (q - member + 4) % 4

    table, gathered = [], []
    for member in range(4):
        i = slot_of(member)
        index = (i + 3) % 4
        is_own = i == 0
        safe = jnp.minimum(index, 2)
        own = (jnp.zeros((8, BLOCK), jnp.int32) + i) == 0
        table.append(jnp.where(own, decay_a[q], table_a[safe]))
        own_tall = (jnp.zeros((wide, BLOCK), jnp.int32) + i) == 0
        gathered.append(
            [
                jnp.where(own_tall, send_a[q, k].astype(f32), recv_a[safe, k].astype(f32))
                for k in range(2)
            ]
        )
    sum_f, through = gathered[0][0], table[0]
    for member in (1, 2, 3):
        sum_f = scaled(sum_f, table[member][:heads], heads) + gathered[member][0]
        through = through * table[member]
    sum_b = gathered[3][1]
    for member in (2, 1, 0):
        sum_b = scaled(sum_b, table[member][heads:], heads) + gathered[member][1]
    send_b[0] = sum_f.astype(bf16)
    send_b[1] = sum_b.astype(bf16)
    decay_b[...] = through
    out_b = []
    for i in range(1, depth):
        to = (z + i) % depth
        lower = (z + i) // depth
        out_b.append(
            remote(
                send_b.at[lower], recv_b.at[i - 1], b_sems.at[0, i - 1], b_sems.at[1, i - 1], tower[i - 1]
            )
        )
        out_b.append(
            remote(
                decay_b, table_b.at[i - 1], b_sems.at[2, i - 1], b_sems.at[3, i - 1], tower[i - 1]
            )
        )
    for copy in out_b:
        copy.start()
    lax.fori_loop(0, groups * blocks // 2, diagonal, 0)
    forward(2, 0)
    for copy in out_b:
        copy.wait_recv()

    carry_f = jnp.zeros((wide, BLOCK), f32)
    carry_b = jnp.zeros((wide, BLOCK), f32)
    for other in range(depth):
        index = (z - other + depth) % depth
        safe = (index + depth - 1) % depth
        safe = jnp.minimum(safe, depth - 2)
        below = (jnp.zeros((wide, BLOCK), jnp.int32) + (z - other)) > 0
        carry_f = jnp.where(
            below, scaled(carry_f, table_b[safe][:heads], heads) + recv_b[safe].astype(f32), carry_f
        )
    for other in reversed(range(depth)):
        index = (z - other + depth) % depth
        safe = (index + depth - 1) % depth
        safe = jnp.minimum(safe, depth - 2)
        above = (jnp.zeros((wide, BLOCK), jnp.int32) + (other - z)) > 0
        carry_b = jnp.where(
            above, scaled(carry_b, table_b[safe][heads:], heads) + recv_b[safe].astype(f32), carry_b
        )
    for member in range(4):
        send_c[member, 0] = carry_f.astype(bf16)
        carry_f = scaled(carry_f, table[member][:heads], heads) + gathered[member][0]
    for member in (3, 2, 1, 0):
        send_c[member, 1] = carry_b.astype(bf16)
        carry_b = scaled(carry_b, table[member][heads:], heads) + gathered[member][1]
    out_c = []
    for i in (1, 2, 3):
        out_c.append(
            remote(
                send_c.at[(q + i) % 4],
                recv_c.at[i - 1],
                c_sems.at[0, i - 1],
                c_sems.at[1, i - 1],
                plane[i - 1],
            )
        )
    for copy in out_c:
        copy.start()
    lax.fori_loop(groups * blocks // 2, groups * blocks, diagonal, 0)
    forward(2, 1)
    for copy in out_c:
        copy.wait_recv()

    def finish(g, carry):
        at_wide = pl.ds(pl.multiple_of(g * wide, wide), wide)
        at_state = pl.ds(pl.multiple_of(g * STATE, STATE), STATE)
        index = (q - g + 4) % 4
        safe = jnp.minimum((index + 3) % 4, 2)
        own = (jnp.zeros((wide, BLOCK), jnp.int32) + index) == 0
        state = [
            jnp.where(own, send_c[q, k].astype(f32), recv_c[safe, k].astype(f32)) for k in range(2)
        ]
        state_f, state_b = state
        for b in range(blocks):
            entering[b, 0] = state_f.astype(bf16)
            state_f = scaled(state_f, passing[g, b][:heads], heads) + fresh[g, b, 0]
        for b in reversed(range(blocks)):
            entering[b, 1] = state_b.astype(bf16)
            state_b = scaled(state_b, passing[g, b][heads:], heads) + fresh[g, b, 1]

        def block(b, inner):
            at_rows = pl.ds(pl.multiple_of(b * BLOCK, BLOCK), BLOCK)
            read, turned = reads[at_rows, at_state], columns[g, b]
            total = within[at_rows, at_wide]
            for k in range(2):
                carried = lax.dot_general(
                    read, entering[b, k], (((1,), (1,)), ((), ())), preferred_element_type=f32
                )
                total = total + carried * spread_heads(turned, (2 + k) * heads, heads, left_lane)
            gate = gate_in[at_rows, at_wide].astype(f32)
            total = total * (gate / (1.0 + jnp.exp(-gate)))
            mean = jnp.mean(total * total, axis=1, keepdims=True)
            total = total * lax.rsqrt(mean + norm_eps) * gain_ref[:, at_wide]
            normed[at_rows, at_wide] = total.astype(bf16)
            return inner

        lax.fori_loop(0, blocks, block, 0)

        @pl.when(g == 1)
        def _():
            forward(3, 0)

        return carry

    for copy in loads[3:6]:
        copy.wait()
    lax.fori_loop(0, groups, finish, 0)

    width = out_ref.shape[1]
    strip = width // 2

    def project(owner_of, store):
        def body(i, carry):
            columns = pl.ds(pl.multiple_of(i * strip, strip), strip)
            taken = pl.ds(pl.multiple_of(owner_of * width + i * strip, strip), strip)
            value = jnp.dot(normed[...], out_weight[:, taken], preferred_element_type=f32)
            store(columns, value.astype(bf16))
            return carry

        lax.fori_loop(0, width // strip, body, 0)

    sums_out = remote(values, recv_o, first_sems.at[0], first_sems.at[1], twin)

    def store_sent(columns, value):
        values[:, columns] = value

    def store_own(columns, value):
        within[:, columns] = resid_scale * stream_in[:, columns].astype(f32) + value.astype(f32)

    project(1 - me, store_sent)
    sums_out.start()
    project(me, store_own)
    forward(3, 1)
    sums_out.wait_recv()
    for b in range(blocks):
        at = pl.ds(b * BLOCK, BLOCK)
        within[at, :] += recv_o[at, :].astype(f32)

    def store_out(at, value):
        out_ref[at, :] = value

    stats = first_sems.at[pl.ds(2, 2)]
    twin_norm(remote, twin, within, mixer_gain_ref, store_out, send_s, recv_s, stats)
    sums_out.wait_send()

    @pl.when(place + 1 < count)
    def _():
        for copy in upward:
            copy.wait_send()

    @pl.when(place > 0)
    def _():
        for copy in downward:
            copy.wait_send()

    forward(4, 0)
    forward(4, 1)
    swap_down.wait()
    swap_up.wait_send()
    for copy in out_a + out_b + out_c + list(flights.values()):
        copy.wait_send()


def state_mixer(
    value_rows,
    entry_rows,
    read_rows,
    gate_rows,
    step_rows,
    sudden,
    rate,
    bias,
    index,
    value_taps,
    entry_taps,
    read_taps,
    gain,
    down,
    up,
    stream,
    out_weight,
    mixer_gain,
):
    height, value_width = value_rows.shape
    state_width = entry_rows.shape[1]
    groups = state_width // STATE
    heads = step_rows.shape[0] // groups
    pairs = 2 * heads
    wide = heads * HEAD_DIM
    blocks = height // BLOCK
    depth = lax.axis_size("sp") // 4
    edge = 16
    dma = pltpu.SemaphoreType.DMA
    vmem, anywhere = pl.BlockSpec(memory_space=pltpu.VMEM), pl.BlockSpec(memory_space=pl.ANY)
    return pl.pallas_call(
        states_kernel,
        out_shape=(
            jax.ShapeDtypeStruct((height, value_width), bf16),
            jax.ShapeDtypeStruct((down.shape[0], down.shape[1] // 2), bf16),
            jax.ShapeDtypeStruct((4 * depth, up.shape[0], up.shape[1] // 2), bf16),
        ),
        in_specs=[anywhere] * 6 + [vmem] * 7 + [anywhere] * 4 + [vmem],
        out_specs=(vmem, anywhere, anywhere),
        scratch_shapes=[
            pltpu.VMEM((height, value_width), bf16),
            pltpu.VMEM((height, state_width), bf16),
            pltpu.VMEM((height, state_width), bf16),
            pltpu.VMEM((height, value_width), bf16),
            pltpu.VMEM(stream.shape, bf16),
            pltpu.VMEM(out_weight.shape, bf16),
            pltpu.VMEM((height, value_width), bf16),
            pltpu.VMEM((height, value_width), bf16),
            pltpu.VMEM((height, 128), f32),
            pltpu.VMEM((height, 128), f32),
            pltpu.VMEM(step_rows.shape, bf16),
            pltpu.VMEM(sudden.shape, f32),
            pltpu.VMEM((BLOCK, BLOCK), f32),
            pltpu.VMEM((groups, pairs, height), f32),
            pltpu.VMEM((groups, pairs, height), f32),
            pltpu.VMEM((blocks, 8, BLOCK), f32),
            pltpu.VMEM((height, BLOCK), f32),
            pltpu.VMEM((height + 16, wide), f32),
            pltpu.VMEM((edge, value_width), bf16),
            pltpu.VMEM((edge, state_width), bf16),
            pltpu.VMEM((edge, state_width), bf16),
            pltpu.VMEM((edge, value_width), bf16),
            pltpu.VMEM((edge, state_width), bf16),
            pltpu.VMEM((edge, state_width), bf16),
            pltpu.VMEM((height, value_width), bf16),
            pltpu.VMEM((height, state_width), bf16),
            pltpu.VMEM((height, state_width), bf16),
            pltpu.VMEM((groups, blocks, 2, wide, STATE), f32),
            pltpu.VMEM((groups, blocks, 4 * heads, BLOCK), f32),
            pltpu.VMEM((groups, blocks, BLOCK, BLOCK), f32),
            pltpu.VMEM((groups, blocks, pairs, BLOCK), f32),
            pltpu.VMEM((height, value_width), f32),
            pltpu.VMEM((blocks, 2, wide, STATE), bf16),
            pltpu.VMEM((groups, 2, wide, STATE), bf16),
            pltpu.VMEM((groups, pairs, BLOCK), f32),
            pltpu.VMEM((3, 2, wide, STATE), bf16),
            pltpu.VMEM((3, pairs, BLOCK), f32),
            pltpu.VMEM((2, wide, STATE), bf16),
            pltpu.VMEM((pairs, BLOCK), f32),
            pltpu.VMEM((depth - 1, wide, STATE), bf16),
            pltpu.VMEM((depth - 1, pairs, BLOCK), f32),
            pltpu.VMEM((4, 2, wide, STATE), bf16),
            pltpu.VMEM((3, 2, wide, STATE), bf16),
            dma((4, 3)),
            dma((4, 3)),
            dma((4, depth - 1)),
            dma((2, 3)),
            dma((4,)),
            dma((2, 2 * depth)),
            dma((2, 2 * depth)),
            dma((8,)),
            dma((4,)),
        ],
        compiler_params=pltpu.CompilerParams(
            collective_id=1, has_side_effects=True, vmem_limit_bytes=56 * 1024 * 1024
        ),
        cost_estimate=pl.CostEstimate(
            flops=60000000000, bytes_accessed=20000000, transcendentals=0
        ),
    )(
        value_rows,
        entry_rows,
        read_rows,
        gate_rows,
        step_rows,
        sudden,
        rate,
        bias,
        index,
        value_taps,
        entry_taps,
        read_taps,
        gain,
        down,
        up,
        stream,
        out_weight,
        mixer_gain,
    )


def plain_states(
    head_value_rows,
    entry_map_rows,
    readout_map_rows,
    output_gate_rows,
    step_before_softplus,
    sudden_log_decay,
    document_index,
    head_rate_logarithm,
    head_step_bias,
    value_conv_taps,
    entry_conv_taps,
    readout_conv_taps,
    group_norm_gain,
):
    rows = head_value_rows.shape[0]
    heads = step_before_softplus.shape[1]
    groups = entry_map_rows.shape[1] // STATE
    per_group = heads // groups
    value_width = head_value_rows.shape[1]
    state_width = entry_map_rows.shape[1]
    blocks = rows // BLOCK
    sp_count = lax.axis_size("sp")
    place = lax.axis_index("sp")
    position = place * rows

    taps = value_conv_taps.shape[0]
    half = taps // 2
    ends = jnp.concatenate(
        [
            jnp.concatenate([a[rows - half :], a[:half]], axis=0)
            for a in (head_value_rows, entry_map_rows, readout_map_rows)
        ],
        axis=1,
    )
    low_all = shifted(ends[:half], 1)
    high_all = shifted(ends[half:], -1)
    doc_pad = jnp.pad(document_index, half + 1, constant_values=-1)
    window_ids = lax.dynamic_slice_in_dim(doc_pad, position + 1, rows + 2 * half)
    own_ids = window_ids[half : half + rows]
    prev_id = window_ids[half - 1]
    next_id = window_ids[half + rows]

    def conv(array, weights, start):
        width = array.shape[1]
        extended = jnp.concatenate(
            [low_all[:, start : start + width], array, high_all[:, start : start + width]], axis=0
        )
        weights = weights.astype(f32)
        total = weights[half] * array.astype(f32)
        for offset in range(taps):
            if offset == half:
                continue
            same = (window_ids[offset : offset + rows] == own_ids)[:, None]
            total = total + weights[offset] * jnp.where(
                same, extended[offset : offset + rows].astype(f32), 0.0
            )
        return jax.nn.silu(total).astype(bf16)

    values = conv(head_value_rows, value_conv_taps, 0)
    entries = conv(entry_map_rows, entry_conv_taps, value_width)
    readout = conv(readout_map_rows, readout_conv_taps, value_width + state_width)
    values = values.reshape(blocks, BLOCK, groups, per_group, HEAD_DIM)
    entries = entries.reshape(blocks, BLOCK, groups, STATE)
    readout = readout.reshape(blocks, BLOCK, groups, STATE)

    raw = step_before_softplus.astype(f32).T
    steps = jax.nn.softplus(raw[None] + head_step_bias[:, :, None])
    decay = -jnp.exp(head_rate_logarithm)[:, :, None] * steps + sudden_log_decay.T[None]
    shape = (2, groups, per_group, blocks, BLOCK)
    steps = jnp.transpose(steps.reshape(shape), (0, 3, 1, 2, 4))
    decay = jnp.transpose(decay.reshape(shape), (0, 3, 1, 2, 4))
    at = lax.iota(jnp.int32, BLOCK)
    upto = (at[:, None] <= at[None, :]).astype(f32)
    running = jnp.einsum("kbgrs,st->kbgrt", decay, upto, precision=exact_prec)
    totals = running[..., -1]
    ahead = running[0]
    behind = running[1] - decay[1]

    ids = own_ids.reshape(blocks, BLOCK)
    first_ids, last_ids = ids[:, 0], ids[:, -1]
    before = jnp.concatenate([prev_id[None], last_ids[:-1]])
    after = jnp.concatenate([first_ids[1:], next_id[None]])
    pass_f = jnp.where((before == last_ids)[:, None, None], jnp.exp(totals[0]), 0.0)
    pass_b = jnp.where((after == first_ids)[:, None, None], jnp.exp(totals[1]), 0.0)
    end_f = jnp.where(
        (ids == last_ids[:, None])[:, None, None], jnp.exp(totals[0][..., None] - ahead), 0.0
    ) * steps[0]
    end_b = jnp.where((ids == first_ids[:, None])[:, None, None], jnp.exp(behind), 0.0) * steps[1]
    arrive_f = jnp.where((ids == before[:, None])[:, None, None], jnp.exp(ahead), 0.0)
    arrive_b = jnp.where(
        (ids == after[:, None])[:, None, None], jnp.exp(totals[1][..., None] - behind), 0.0
    )

    own_f, own_b = jnp.prod(pass_f, axis=0), jnp.prod(pass_b, axis=0)

    def fresh_states(weight):
        weighted = values.astype(f32) * jnp.transpose(weight, (0, 3, 1, 2))[..., None]
        return jnp.einsum(
            "bsgrp,bsgn->bgrpn", weighted.astype(bf16), entries, preferred_element_type=f32
        )

    fresh_f = fresh_states(end_f)
    fresh_b = fresh_states(end_b)

    end_state = fresh_f[0]
    for b in range(1, blocks):
        end_state = end_state * pass_f[b][..., None, None] + fresh_f[b]
    start_state = fresh_b[blocks - 1]
    for b in range(blocks - 2, -1, -1):
        start_state = start_state * pass_b[b][..., None, None] + fresh_b[b]
    reach = -(-LONGEST_DOCUMENT // rows)
    in_f = incoming_state(end_state, own_f, 1, reach)
    in_b = incoming_state(start_state, own_b, -1, reach)

    scores = jnp.einsum("btgn,bsgn->bgts", readout, entries, preferred_element_type=f32)
    later = at[:, None] > at[None, :]
    equal = at[:, None] == at[None, :]
    linked = (ids[:, :, None] == ids[:, None, :])[:, None, None]
    spread = jnp.where(
        later,
        ahead[..., :, None] - ahead[..., None, :],
        behind[..., None, :] - behind[..., :, None],
    )
    strength = jnp.where(
        later,
        steps[0][..., None, :],
        jnp.where(equal, steps[0][..., None, :], 0.0) + steps[1][..., None, :],
    )
    weights = jnp.where(linked, jnp.exp(spread) * strength, 0.0)
    mixing = (scores[:, :, None] * weights).astype(bf16)
    output = jnp.einsum("bgrts,bsgrp->bgrtp", mixing, values, preferred_element_type=f32)

    state_f = [in_f]
    for b in range(blocks - 1):
        state_f.append(state_f[-1] * pass_f[b][..., None, None] + fresh_f[b])
    state_b = [in_b]
    for b in range(blocks - 1, 0, -1):
        state_b.append(state_b[-1] * pass_b[b][..., None, None] + fresh_b[b])
    entering_f = jnp.stack([s.astype(bf16) for s in state_f])
    entering_b = jnp.stack([s.astype(bf16) for s in state_b[::-1]])
    carried_f = jnp.einsum("btgn,bgrpn->bgrtp", readout, entering_f, preferred_element_type=f32)
    carried_b = jnp.einsum("btgn,bgrpn->bgrtp", readout, entering_b, preferred_element_type=f32)
    output = output + carried_f * arrive_f[..., None] + carried_b * arrive_b[..., None]

    gated = jnp.transpose(output, (0, 3, 1, 2, 4)).reshape(rows, groups, per_group * HEAD_DIM)
    gated = gated * jax.nn.silu(output_gate_rows.astype(f32)).reshape(gated.shape)
    gated = gated * lax.rsqrt(jnp.mean(gated * gated, axis=2, keepdims=True) + norm_eps)
    normed = (gated.reshape(rows, value_width) * group_norm_gain).astype(bf16)
    return normed


def ring_states(
    head_value_rows,
    entry_map_rows,
    readout_map_rows,
    output_gate_rows,
    step_before_softplus,
    sudden_log_decay,
    document_index,
    head_rate_logarithm,
    head_step_bias,
    value_conv_taps,
    entry_conv_taps,
    readout_conv_taps,
    group_norm_gain,
    *dense,
):
    return state_mixer(
        head_value_rows,
        entry_map_rows,
        readout_map_rows,
        output_gate_rows,
        step_before_softplus.T,
        sudden_log_decay.T,
        head_rate_logarithm,
        head_step_bias,
        document_index.reshape(-1, BLOCK),
        value_conv_taps,
        entry_conv_taps,
        readout_conv_taps,
        group_norm_gain[None],
        *dense,
    )


def per_device(
    head_value_rows,
    entry_map_rows,
    readout_map_rows,
    output_gate_rows,
    step_before_softplus,
    sudden_log_decay,
    document_index,
    head_rate_logarithm,
    head_step_bias,
    value_conv_taps,
    entry_conv_taps,
    readout_conv_taps,
    group_norm_gain,
    mixer_output_weight,
    stream,
    mixer_norm_gain,
    channel_norm_gain,
    up_projection_weight,
    down_projection_weight,
):
    model_width = mixer_output_weight.shape[1]
    rows = head_value_rows.shape[0]
    inputs = (
        head_value_rows,
        entry_map_rows,
        readout_map_rows,
        output_gate_rows,
        step_before_softplus,
        sudden_log_decay,
        document_index,
        head_rate_logarithm,
        head_step_bias,
        value_conv_taps,
        entry_conv_taps,
        readout_conv_taps,
        group_norm_gain,
    )
    if has_rings() and entry_map_rows.shape[1] == 4 * STATE:
        normed_one, other, up_all = ring_states(
            *inputs,
            down_projection_weight,
            up_projection_weight,
            stream,
            mixer_output_weight,
            mixer_norm_gain[None],
        )
        return ring_mixer(
            normed_one,
            channel_norm_gain[None],
            down_projection_weight,
            other,
            up_projection_weight,
            up_all,
        )
    up_half, down_half = pair_weights(up_projection_weight), pair_weights(down_projection_weight)
    normed = plain_states(*inputs)
    mixer_sum = tp_scatter(jnp.dot(normed, mixer_output_weight, preferred_element_type=f32))
    first_sum = resid_scale * stream.astype(f32) + mixer_sum
    normed_one = norm_rows(first_sum, mixer_norm_gain, model_width)
    piece = rows // PIECES
    returned = [
        pair_swap(
            channel_mixer(
                pair_swap(normed_one[i * piece : (i + 1) * piece]),
                up_half,
                down_half,
            ).astype(bf16)
        )
        for i in range(PIECES)
    ]
    down_sum = channel_mixer(normed_one, up_half, down_half) + jnp.concatenate(returned).astype(f32)
    second_sum = resid_scale * normed_one.astype(f32) + down_sum
    return norm_rows(second_sum, channel_norm_gain, model_width)


def solution(mesh):
    placed = (
        P("sp", "tp"),
        P("sp", "tp"),
        P("sp", "tp"),
        P("sp", "tp"),
        P("sp", "tp"),
        P("sp", "tp"),
        P(),
        P(None, "tp"),
        P(None, "tp"),
        P(None, "tp"),
        P(None, "tp"),
        P(None, "tp"),
        P("tp"),
        P("tp", None),
        P("sp", "tp"),
        P("tp"),
        P("tp"),
        P("sp", "tp"),
        P("sp", "tp"),
    )
    return jax.shard_map(
        per_device, mesh=mesh, in_specs=placed, out_specs=P("sp", "tp"), check_vma=False
    )
```
